32 devices in a mesh: grp: 2 (over y), fs: 4 (over z), tp: 4 (over x, core).
Axes of the slice: x: 2, y: 2, z: 4, core: 2. Of those that a mesh axis runs over, the one named last changes fastest.
Arguments:
- tokens: bfloat16 [2560, 2048], P(('grp', 'fs', 'tp')), parts along dimension 0, may hold values from -6 to 6
- mix_gain: bfloat16 [2048], replicated, may hold values from 0.099609375 to 1.8984375
- val_weight: bfloat16 [2048, 1024], P('fs', 'tp'), may hold values from -4 to 4
- gate_weight: bfloat16 [2048, 1024], P('fs', 'tp'), may hold values from -0.125 to 0.125
- conv_taps: bfloat16 [31, 1024], replicated, may hold values from -1 to 1
- chan_gain: bfloat16 [1024], replicated, may hold values from 0.099609375 to 1.8984375
- out_weight: bfloat16 [1024, 2048], P('tp', 'fs'), may hold values from -0.1875 to 0.1875
- mix_post_gain: bfloat16 [2048], replicated, may hold values from 0.099609375 to 1.8984375
- ffn_gain: bfloat16 [2048], replicated, may hold values from 0.099609375 to 1.8984375
- up_gate_weight: bfloat16 [2048, 5120], P('fs', 'tp'), may hold values from -0.125 to 0.125
- up_val_weight: bfloat16 [2048, 5120], P('fs', 'tp'), may hold values from -0.125 to 0.125
- ffn_taps: bfloat16 [2, 3, 5120], replicated, may hold values from -3.5 to 3.5
- down_weight: bfloat16 [5120, 2048], P('tp', 'fs'), may hold values from -0.078125 to 0.078125
- ffn_post_gain: bfloat16 [2048], replicated, may hold values from 0.099609375 to 1.8984375
Outputs:
- layer_out: bfloat16 [2560, 2048], P(('grp', 'fs', 'tp')), parts along dimension 0
The draws below stay inside these ranges and needn't reach their ends.
There are 2 independent parts, one for each index of `grp`. The reference program is written for one: setup_inputs(seed, part) draws one part's arguments, and reference() takes and returns one part's arrays. A program takes and returns all parts, laid end to end along the dimension named above; an argument that names none is the same for every part. Nothing has to cross between parts.
All inputs are finite; a program needn't handle non-finite values.
Results may differ from the reference program's by a relative error of at most 0.019.
Values may be sent and summed in bfloat16 or wider, within the bound.
No kernel may reach another device: no remote copies, remote signals or barrier semaphores. Data moves between devices by JAX's collectives and lax.ppermute only.
A program may use at most 64 MiB of HBM per device.

```python
import jax
import jax.numpy as jnp
from jax import lax

D = 2048
CH = 1024
FF = 5120
CONV_TAPS = 31
FFN_TAPS = 3
LEN = 64
TOKENS = 1280
N_TP = 4


def draw_val_weight(key, part):
    base_key, rough_key = jax.random.split(key, 2)
    base_draw = jax.random.normal(base_key, (D, CH), jnp.float32) * D ** (-0.5)
    roughness = jnp.exp(jax.random.uniform(rough_key, (CH,), jnp.float32, -0.7, 0.7))
    position = jnp.arange(CH, dtype=jnp.float32) / CH
    drawn_values = base_draw * 4.0 ** position * roughness
    return jnp.clip(drawn_values, -4.0, 4.0).astype(jnp.bfloat16)


def shard_levels(rng, dims, pieces, smallest, top_value):
    level = 1.0
    for dim, shards_of in pieces:
        steps = jax.random.uniform(jax.random.fold_in(jax.random.fold_in(rng, 6), dim), (shards_of,), jnp.float32, smallest / len(pieces), top_value / len(pieces))
        level = level * jnp.repeat(jnp.exp(steps), dims[dim] // shards_of).reshape((-1,) + (1,) * (len(dims) - 1 - dim))
    return level


def gaussian(rng, shape, scale, most, cuts=(), held_as=jnp.bfloat16):
    values = jax.random.normal(rng, shape, jnp.float32) * scale
    if len(cuts) > 0:
        values = shard_levels(rng, shape, cuts, -0.22, 0.18) * values
    return jnp.clip(values, min=-most, max=most).astype(held_as)


def setup_inputs(seed: int = 0, part: int = 0) -> dict:
    splits = jax.random.split(jax.random.key(seed), 15)
    part_splits = jax.random.split(jax.random.fold_in(splits[14], part), 15)
    return {
        "tokens": gaussian(part_splits[0], (TOKENS, D), 1.0, 6.0, ((0, 16),)),
        "mix_gain": jnp.clip(1.0 + 0.18 * jax.random.normal(splits[1], (D,), jnp.float32), 0.099609375, 1.8984375).astype(jnp.bfloat16),
        "val_weight": draw_val_weight(jax.random.fold_in(splits[14], 71), part),
        "gate_weight": gaussian(splits[3], (D, CH), D ** -0.5, 0.125, ((0, 4), (1, 4))),
        "conv_taps": gaussian(splits[4], (CONV_TAPS, CH), CONV_TAPS ** -0.5, 1.0),
        "chan_gain": jnp.clip(1.0 + 0.18 * jax.random.normal(splits[5], (CH,), jnp.float32), 0.099609375, 1.8984375).astype(jnp.bfloat16),
        "out_weight": gaussian(splits[6], (CH, D), CH ** -0.5, 0.1875, ((0, 4), (1, 4))),
        "mix_post_gain": jnp.clip(1.0 + 0.18 * jax.random.normal(splits[7], (D,), jnp.float32), 0.099609375, 1.8984375).astype(jnp.bfloat16),
        "ffn_gain": jnp.clip(1.0 + 0.18 * jax.random.normal(splits[8], (D,), jnp.float32), 0.099609375, 1.8984375).astype(jnp.bfloat16),
        "up_gate_weight": gaussian(splits[9], (D, FF), D ** -0.5, 0.125, ((0, 4), (1, 4))),
        "up_val_weight": gaussian(splits[10], (D, FF), D ** -0.5, 0.125, ((0, 4), (1, 4))),
        "ffn_taps": gaussian(splits[11], (2, FFN_TAPS, FF), FFN_TAPS ** -0.5, 3.5),
        "down_weight": gaussian(splits[12], (FF, D), FF ** -0.5, 0.078125, ((0, 4), (1, 4))),
        "ffn_post_gain": jnp.clip(1.0 + 0.18 * jax.random.normal(splits[13], (D,), jnp.float32), 0.099609375, 1.8984375).astype(jnp.bfloat16),
    }


norm_epsilon = 1e-06
chan_epsilon = 1e-05

def rms_scale(values, gain):
    inverse = lax.rsqrt(lax.optimization_barrier(jnp.mean(values * values, axis=-1, keepdims=True)) + norm_epsilon)
    return values * inverse * gain.astype(jnp.float32)

def depthwise(signal, tap_table):
    taps_count = tap_table.shape[0]
    channels = signal.shape[1]
    shaped = signal.astype(jnp.float32).reshape(signal.shape[0] // LEN, LEN, channels)
    padded = jnp.pad(shaped, ((0, 0), (taps_count - 1, 0), (0, 0)))
    tap_values = tap_table.astype(jnp.float32)
    result = jnp.zeros(shaped.shape, jnp.float32)
    for offset in range(taps_count):
        result = result + padded[:, offset:offset + LEN, :] * tap_values[offset]
    return result.reshape(signal.shape[0], channels)

def grouped_sum(left, weight):
    group_width = left.shape[1] // N_TP

    def step(running, group_index):
        columns = lax.dynamic_slice_in_dim(left, group_index * group_width, group_width, 1)
        row_block = lax.dynamic_slice_in_dim(weight, group_index * group_width, group_width, 0)
        partial_value = jnp.dot(columns, row_block, preferred_element_type=jnp.float32).astype(jnp.bfloat16)
        partial_value = lax.optimization_barrier(partial_value)
        return (running + partial_value.astype(jnp.float32), None)
    start_sum = jnp.zeros((left.shape[0], weight.shape[1]), jnp.float32)
    running, _ = lax.scan(step, start_sum, jnp.arange(N_TP, dtype=jnp.int32))
    return running

def reference(tokens, mix_gain, val_weight, gate_weight, conv_taps, chan_gain, out_weight, mix_post_gain, ffn_gain, up_gate_weight, up_val_weight, ffn_taps, down_weight, ffn_post_gain):
    normed = rms_scale(tokens.astype(jnp.float32), mix_gain).astype(jnp.bfloat16)
    values = jnp.dot(normed, val_weight, preferred_element_type=jnp.float32)
    gate_sums = jnp.dot(normed, gate_weight, preferred_element_type=jnp.float32)
    glu_out = (values * jax.nn.sigmoid(gate_sums)).astype(jnp.bfloat16)
    conv_out = depthwise(glu_out, conv_taps)
    chan_mean = lax.optimization_barrier(jnp.mean(conv_out, axis=-1, keepdims=True))
    chan_var = lax.optimization_barrier(jnp.mean(conv_out * conv_out, axis=-1, keepdims=True)) - chan_mean * chan_mean
    scaled = (conv_out - chan_mean) * lax.rsqrt(chan_var + chan_epsilon) * chan_gain.astype(jnp.float32)
    activated = jax.nn.silu(scaled).astype(jnp.bfloat16)
    mixed_sum = grouped_sum(activated, out_weight)
    residual = (tokens.astype(jnp.float32) + rms_scale(mixed_sum, mix_post_gain)).astype(jnp.bfloat16)
    normed_ffn = rms_scale(residual.astype(jnp.float32), ffn_gain).astype(jnp.bfloat16)
    up_gate = jnp.dot(normed_ffn, up_gate_weight, preferred_element_type=jnp.float32).astype(jnp.bfloat16)
    up_val = jnp.dot(normed_ffn, up_val_weight, preferred_element_type=jnp.float32).astype(jnp.bfloat16)
    gate_conv = depthwise(up_gate, ffn_taps[0])
    val_conv = depthwise(up_val, ffn_taps[1])
    hidden = (jax.nn.gelu(gate_conv, approximate=True) * val_conv).astype(jnp.bfloat16)
    ffn_sum = grouped_sum(hidden, down_weight)
    return (residual.astype(jnp.float32) + rms_scale(ffn_sum, ffn_post_gain)).astype(jnp.bfloat16)
```

```python
import jax
import jax.numpy as jnp
from jax import lax
from jax.experimental import pallas as pl
from jax.experimental.pallas import tpu as pltpu
from jax.sharding import PartitionSpec as P

LEN = 64
LANES = 128

norm_epsilon = 1e-06
chan_epsilon = 1e-05


def rms_scale(values, gain):
    inverse = lax.rsqrt(jnp.mean(values * values, axis=-1, keepdims=True) + norm_epsilon)
    return values * inverse * gain.astype(jnp.float32)


def depthwise(signal, tap_table):
    taps_count = tap_table.shape[0]
    channels = signal.shape[1]
    shaped = signal.astype(jnp.float32).reshape(signal.shape[0] // LEN, LEN, channels)
    padded = jnp.pad(shaped, ((0, 0), (taps_count - 1, 0), (0, 0)))
    tap_values = tap_table.astype(jnp.float32)
    result = jnp.zeros(shaped.shape, jnp.float32)
    for offset in range(taps_count):
        result = result + padded[:, offset : offset + LEN, :] * tap_values[offset]
    return result.reshape(signal.shape[0], channels)


def product(left, weight):
    return jnp.dot(left, weight, preferred_element_type=jnp.float32)


def swap(array, axis, size, bits):
    return lax.ppermute(array, axis, [(i, i ^ bits) for i in range(size)])


def pick(array, *indices):
    for index in indices:
        array = lax.dynamic_index_in_dim(array, index, 0, keepdims=False)
    return array


def put(array, piece, *indices):
    missing = array.ndim - len(indices)
    piece = piece.reshape((1,) * len(indices) + array.shape[len(indices) :])
    return lax.dynamic_update_slice(array, piece, (*indices, *([0] * missing)))


def gather_blocks(block, axis, size):
    blocks = {0: block}
    bits = size // 2
    while bits:
        blocks.update({d ^ bits: swap(b, axis, size, bits) for d, b in list(blocks.items())})
        bits //= 2
    return blocks


def scatter_blocks(blocks, axis, size):
    bits = 1
    while bits < size:
        kept = {}
        for d in blocks:
            if not d & bits:
                other = swap(blocks[d | bits], axis, size, bits)
                kept[d] = blocks[d].astype(jnp.float32) + other.astype(jnp.float32)
        bits *= 2
        if bits < size:
            kept = {d: b.astype(jnp.bfloat16) for d, b in kept.items()}
        blocks = kept
    return blocks[0]


def ffn_chunk(member, blocks, up, taps, down):
    count = len(blocks)
    rows, width = blocks[0].shape
    total = count * rows
    packed = up.shape[1]
    parts, units, out_cols = down.shape
    whole = units // LANES * LANES
    rest = units - whole

    def body(member_ref, *refs):
        block_refs = refs[:count]
        up_ref, taps_ref, down_ref = refs[count : count + 3]
        out_refs = refs[count + 3 : 2 * count + 3]
        gathered, hidden, mixed = refs[2 * count + 3 :]
        here = member_ref[0]
        for d in range(count):
            gathered[pl.ds(pl.multiple_of((here ^ d) * rows, 16), rows), :] = block_refs[d][...]
        place = lax.broadcasted_iota(jnp.int32, (total, LANES), 0) % LEN

        def conv(column):
            columns = pl.ds(column, LANES)
            raw = product(gathered[...], up_ref[:, columns])
            raw = raw.astype(jnp.bfloat16).astype(jnp.float32)
            depth = taps_ref.shape[0]
            result = raw * taps_ref[depth - 1 : depth, columns]
            for back in range(1, depth):
                moved = jnp.where(place >= back, pltpu.roll(raw, back, 0), 0.0)
                result = result + moved * taps_ref[depth - 1 - back : depth - back, columns]
            return result

        def gelu(v):
            return 0.5 * v * (1.0 + jnp.tanh((2.0 / jnp.pi) ** 0.5 * (v + 0.044715 * v * v * v)))

        for column in range(0, whole, LANES):
            gate, val = conv(column), conv(whole + column)
            hidden[:, column : column + LANES] = (gelu(gate) * val).astype(jnp.bfloat16)
        if rest:
            both = conv(2 * whole)
            lane = lax.broadcasted_iota(jnp.int32, (total, LANES), 1)
            prod = gelu(both) * pltpu.roll(both, LANES - rest, 1)
            hidden[:, whole:] = jnp.where(lane < rest, prod, 0.0).astype(jnp.bfloat16)
        for part in range(parts):
            columns = pl.ds(part * out_cols, out_cols)
            out = product(hidden[:, :units], down_ref[part])
            mixed[:, columns] = out.astype(jnp.bfloat16)
        for d in range(count):
            out_refs[d][...] = mixed[pl.ds(pl.multiple_of((here ^ d) * rows, 16), rows), :]

    vmem = pl.BlockSpec(memory_space=pltpu.VMEM)
    out = jax.ShapeDtypeStruct((rows, parts * out_cols), jnp.bfloat16)
    flops = 2 * total * width * packed + 2 * total * units * parts * out_cols
    return pl.pallas_call(
        body,
        in_specs=[pl.BlockSpec(memory_space=pltpu.SMEM)] + [vmem] * (count + 3),
        out_specs=[vmem] * count,
        out_shape=[out] * count,
        scratch_shapes=[
            pltpu.VMEM((total, width), jnp.bfloat16),
            pltpu.VMEM((total, whole + (LANES if rest else 0)), jnp.bfloat16),
            pltpu.VMEM((total, parts * out_cols), jnp.bfloat16),
        ],
        cost_estimate=pl.CostEstimate(
            flops=flops, transcendentals=total * units, bytes_accessed=up.size * 2
        ),
        name="ffn_chunk",
    )(member, *[blocks[d] for d in range(count)], up, taps, down)


def exchange_shards(sizes):
    ng, nf, nt = sizes

    def shards(
        tokens,
        mix_gain,
        val_weight,
        gate_weight,
        conv_taps,
        chan_gain,
        out_weight,
        mix_post_gain,
        ffn_gain,
        up_gate_weight,
        up_val_weight,
        ffn_taps,
        down_weight,
        ffn_post_gain,
    ):
        group, slab, member = (lax.axis_index(a) for a in ("grp", "fs", "tp"))
        rows, width = tokens.shape

        def halves(array):
            return array.reshape(ng, array.shape[0] // ng, array.shape[1])

        def fetch(piece_for, target):
            for d in range(1, nf):
                piece = swap(piece_for(d), "fs", nf, d)
                target = put(target, piece, slab ^ d, group)
                for e in range(1, ng):
                    other = swap(piece, "grp", ng, e)
                    target = put(target, other, slab ^ d, group ^ e)
            return target

        def gathered(array):
            own = halves(array)
            mine = pick(own, group)
            start = jnp.broadcast_to(own[None], (nf,) + own.shape)
            return fetch(lambda d: mine, start)

        local_ch = val_weight.shape[1]
        glu_weight = gathered(jnp.concatenate([val_weight, gate_weight], axis=1))
        glu_weight = glu_weight.reshape(nf * val_weight.shape[0], 2 * local_ch)
        out_full = gathered(out_weight).reshape(nf, *out_weight.shape)
        out_full = jnp.concatenate([out_full[s] for s in range(nf)], axis=1)

        local_ff = up_gate_weight.shape[1]
        units = local_ff // nf
        whole = units // LANES * LANES

        def pack(gate, val):
            def block(s):
                a, b, c = s * units, s * units + whole, (s + 1) * units
                cut = [gate[..., a:b], val[..., a:b], gate[..., b:c], val[..., b:c]]
                return jnp.concatenate(cut, axis=-1)

            return jnp.stack([block(s) for s in range(nf)])

        up_blocks = pack(up_gate_weight, up_val_weight)
        up_blocks = up_blocks.reshape(nf, ng, up_blocks.shape[1] // ng, 2 * units)
        up_full = fetch(lambda d: pick(up_blocks, slab ^ d, group), up_blocks)
        up_full = up_full.reshape(nf * up_gate_weight.shape[0], 2 * units)
        down_blocks = down_weight.reshape(nf, ng, units // ng, down_weight.shape[1])
        down_full = fetch(lambda d: pick(down_blocks, slab ^ d, group), down_blocks)
        down_full = down_full.reshape(nf, units, down_weight.shape[1])
        own_taps = lax.dynamic_slice_in_dim(ffn_taps, member * local_ff, local_ff, 2)
        own_taps = pick(pack(own_taps[0], own_taps[1]), slab).astype(jnp.float32)

        normed_own = rms_scale(tokens.astype(jnp.float32), mix_gain).astype(jnp.bfloat16)
        row_blocks = gather_blocks(normed_own, "tp", nt)
        normed = jnp.zeros((nt, rows, width), jnp.bfloat16)
        for d, b in row_blocks.items():
            normed = put(normed, b, member ^ d)
        normed = normed.reshape(nt * rows, width)
        both = product(normed, glu_weight)
        glu_out = (both[:, :local_ch] * jax.nn.sigmoid(both[:, local_ch:])).astype(jnp.bfloat16)
        mix_taps = lax.dynamic_slice_in_dim(conv_taps, member * local_ch, local_ch, 1)
        conv_out = depthwise(glu_out, mix_taps)
        totals, squares = lax.psum(
            (jnp.sum(conv_out, axis=1), jnp.sum(conv_out * conv_out, axis=1)), "tp"
        )
        all_channels = chan_gain.shape[0]
        chan_mean = totals[:, None] / all_channels
        chan_var = squares[:, None] / all_channels - chan_mean * chan_mean
        own_gain = lax.dynamic_slice_in_dim(chan_gain, member * local_ch, local_ch, 0)
        scaled = (conv_out - chan_mean) * lax.rsqrt(chan_var + chan_epsilon)
        activated = jax.nn.silu(scaled * own_gain.astype(jnp.float32)).astype(jnp.bfloat16)
        mixed = product(activated, out_full).astype(jnp.bfloat16).reshape(nt, rows, width)
        mixed_sum = scatter_blocks({d: pick(mixed, member ^ d) for d in range(nt)}, "tp", nt)
        residual = tokens.astype(jnp.float32) + rms_scale(mixed_sum, mix_post_gain)
        residual = residual.astype(jnp.bfloat16)

        normed_share = rms_scale(residual.astype(jnp.float32), ffn_gain).astype(jnp.bfloat16)
        where = member.astype(jnp.int32).reshape(1)
        ffn_sum = None
        for d in range(nf):
            block = swap(normed_share, "fs", nf, d) if d else normed_share
            blocks = gather_blocks(block, "tp", nt)
            parts = ffn_chunk(where, blocks, up_full, own_taps, down_full)
            part = scatter_blocks(dict(enumerate(parts)), "tp", nt)
            if d:
                part = swap(part.astype(jnp.bfloat16), "fs", nf, d).astype(jnp.float32)
            ffn_sum = part if ffn_sum is None else ffn_sum + part
        result = residual.astype(jnp.float32) + rms_scale(ffn_sum, ffn_post_gain)
        return result.astype(jnp.bfloat16)

    return shards


def gather_shards(
    tokens,
    mix_gain,
    val_weight,
    gate_weight,
    conv_taps,
    chan_gain,
    out_weight,
    mix_post_gain,
    ffn_gain,
    up_gate_weight,
    up_val_weight,
    ffn_taps,
    down_weight,
    ffn_post_gain,
):
    member = lax.axis_index("tp")
    normed_own = rms_scale(tokens.astype(jnp.float32), mix_gain).astype(jnp.bfloat16)
    normed = lax.all_gather(normed_own, "tp", axis=0, tiled=True)
    local_ch = val_weight.shape[1]
    values = product(normed, lax.all_gather(val_weight, "fs", axis=0, tiled=True))
    gate_sums = product(normed, lax.all_gather(gate_weight, "fs", axis=0, tiled=True))
    glu_out = (values * jax.nn.sigmoid(gate_sums)).astype(jnp.bfloat16)
    own_taps = lax.dynamic_slice_in_dim(conv_taps, member * local_ch, local_ch, 1)
    conv_out = depthwise(glu_out, own_taps)
    totals, squares = lax.psum(
        (jnp.sum(conv_out, axis=1), jnp.sum(conv_out * conv_out, axis=1)), "tp"
    )
    all_channels = chan_gain.shape[0]
    chan_mean = totals[:, None] / all_channels
    chan_var = squares[:, None] / all_channels - chan_mean * chan_mean
    own_gain = lax.dynamic_slice_in_dim(chan_gain, member * local_ch, local_ch, 0)
    scaled = (conv_out - chan_mean) * lax.rsqrt(chan_var + chan_epsilon)
    activated = jax.nn.silu(scaled * own_gain.astype(jnp.float32)).astype(jnp.bfloat16)
    out_full = lax.all_gather(out_weight, "fs", axis=1, tiled=True)
    mixed_sum = lax.psum_scatter(
        product(activated, out_full).astype(jnp.bfloat16), "tp", scatter_dimension=0, tiled=True
    ).astype(jnp.float32)
    residual = tokens.astype(jnp.float32) + rms_scale(mixed_sum, mix_post_gain)
    residual = residual.astype(jnp.bfloat16)
    normed_share = rms_scale(residual.astype(jnp.float32), ffn_gain).astype(jnp.bfloat16)
    normed_ffn = lax.all_gather(normed_share, "tp", axis=0, tiled=True)
    local_ff = up_gate_weight.shape[1]
    own_ffn_taps = lax.dynamic_slice_in_dim(ffn_taps, member * local_ff, local_ff, 2)
    gate_full = lax.all_gather(up_gate_weight, "fs", axis=0, tiled=True)
    val_full = lax.all_gather(up_val_weight, "fs", axis=0, tiled=True)
    up_gate = product(normed_ffn, gate_full).astype(jnp.bfloat16)
    up_val = product(normed_ffn, val_full).astype(jnp.bfloat16)
    gate_conv = depthwise(up_gate, own_ffn_taps[0])
    val_conv = depthwise(up_val, own_ffn_taps[1])
    hidden = (jax.nn.gelu(gate_conv, approximate=True) * val_conv).astype(jnp.bfloat16)
    down_full = lax.all_gather(down_weight, "fs", axis=1, tiled=True)
    ffn_sum = lax.psum_scatter(
        product(hidden, down_full).astype(jnp.bfloat16), "tp", scatter_dimension=0, tiled=True
    ).astype(jnp.float32)
    return (residual.astype(jnp.float32) + rms_scale(ffn_sum, ffn_post_gain)).astype(jnp.bfloat16)


def solution(mesh):
    sizes = tuple(mesh.shape[a] for a in ("grp", "fs", "tp"))
    specs = (
        P(("grp", "fs", "tp"), None),
        P(),
        P("fs", "tp"),
        P("fs", "tp"),
        P(),
        P(),
        P("tp", "fs"),
        P(),
        P(),
        P("fs", "tp"),
        P("fs", "tp"),
        P(),
        P("tp", "fs"),
        P(),
    )

    def run(*args):
        powers = all(size & (size - 1) == 0 for size in sizes)
        units = args[9].shape[1] // (sizes[1] * sizes[2])
        cuts = units % LANES in (0, LANES // 2) and units % (16 * sizes[0]) == 0
        few = sizes[1] * sizes[2] <= 16
        shards = exchange_shards(sizes) if powers and cuts and few else gather_shards
        return jax.shard_map(
            shards,
            mesh=mesh,
            in_specs=specs,
            out_specs=P(("grp", "fs", "tp"), None),
            check_vma=False,
        )(*args)

    return run
```

```python
import jax
import jax.numpy as jnp
from jax import lax
from jax.experimental import pallas as pl
from jax.experimental.pallas import tpu as pltpu
from jax.sharding import PartitionSpec as P

LEN = 64
LANES = 128
BF16 = jnp.bfloat16
F32 = jnp.float32
MEBI = 2**20

norm_epsilon = 1e-06
chan_epsilon = 1e-05


def rms_scale(values, gain):
    inverse = lax.rsqrt(jnp.mean(values * values, axis=-1, keepdims=True) + norm_epsilon)
    return values * inverse * gain.astype(jnp.float32)


def depthwise(signal, tap_table):
    taps_count = tap_table.shape[0]
    channels = signal.shape[1]
    shaped = signal.astype(jnp.float32).reshape(signal.shape[0] // LEN, LEN, channels)
    padded = jnp.pad(shaped, ((0, 0), (taps_count - 1, 0), (0, 0)))
    tap_values = tap_table.astype(jnp.float32)
    result = jnp.zeros(shaped.shape, jnp.float32)
    for offset in range(taps_count):
        result = result + padded[:, offset : offset + LEN, :] * tap_values[offset]
    return result.reshape(signal.shape[0], channels)


def product(left, weight):
    return jnp.dot(left, weight, preferred_element_type=jnp.float32)


def swap(array, axis, size, bits):
    return lax.ppermute(array, axis, [(i, i ^ bits) for i in range(size)])


def pick(array, *indices):
    for index in indices:
        array = lax.dynamic_index_in_dim(array, index, 0, keepdims=False)
    return array


def halvings(size):
    return [1 << b for b in reversed(range(size.bit_length() - 1))]


def gather_blocks(block, axis, size):
    blocks = {0: block}
    for bits in halvings(size):
        for d in list(blocks):
            blocks[d | bits] = swap(blocks[d], axis, size, bits)
    return blocks


def scatter_blocks(blocks, axis, size):
    terms = {d: [b] for d, b in blocks.items()}
    for bits in reversed(halvings(size)):
        kept = {}
        for d in terms:
            if not d & bits:
                sent = add_terms(terms[d | bits])
                other = swap(sent, axis, size, bits)
                kept[d] = [*terms[d], other]
        terms = kept
    return terms[0]


def add_terms(terms):
    if len(terms) == 1:
        return terms[0]
    return sum(t.astype(F32) for t in terms).astype(BF16)


VMEM = pl.BlockSpec(memory_space=pltpu.VMEM)
SMEM = pl.BlockSpec(memory_space=pltpu.SMEM)
HBM = pl.BlockSpec(memory_space=pl.ANY)


def aligned(index, size):
    return pl.ds(pl.multiple_of(index * size, 16), size)


def start_copies(pairs, sems, first=0):
    copies = []
    for i, (source, target) in enumerate(pairs):
        copies.append(pltpu.make_async_copy(source, target, sems.at[first + i]))
        copies[-1].start()
    return copies


def row_kernel(body, arrays, outs):
    count = len(arrays)

    def run(*refs):
        results = body(*[ref[...].astype(F32) for ref in refs[:count]])
        for ref, result in zip(refs[count:], results):
            ref[...] = result.astype(ref.dtype)

    return pl.pallas_call(
        run,
        in_specs=[VMEM] * count,
        out_specs=[VMEM] * outs,
        out_shape=[jax.ShapeDtypeStruct(arrays[0].shape, BF16)] * outs,
        cost_estimate=pl.CostEstimate(
            flops=8 * arrays[0].size, transcendentals=0, bytes_accessed=4 * arrays[0].size
        ),
        compiler_params=pltpu.CompilerParams(vmem_limit_bytes=12 * MEBI),
    )(*arrays)


def glu_conv(spot, sizes, blocks, own, pieces, taps):
    ng, nf, nt = sizes
    rows, width = blocks[0].shape
    total = nt * rows
    depth, packed = own.shape
    share = depth // ng
    channels = packed // 2
    count = taps.shape[0]
    lead = -(-(count - 1) // 8) * 8
    segments = total // LEN
    keys = list(pieces)

    def run(spot_ref, taps_ref, *refs):
        block_refs, refs = refs[:nt], refs[nt:]
        own_ref, refs = refs[0], refs[1:]
        piece_refs, refs = refs[: len(keys)], refs[len(keys) :]
        conv_ref, sums_ref, gathered, weight, padded, sems = refs
        group, slab, member = spot_ref[0], spot_ref[1], spot_ref[2]
        pairs = [(block_refs[d], gathered.at[aligned(member ^ d, rows)]) for d in range(nt)]
        pairs.append((own_ref, weight.at[aligned(slab, depth)]))
        for (d, e), ref in zip(keys, piece_refs):
            place = (slab ^ d) * ng + (group ^ e)
            pairs.append((ref, weight.at[aligned(place, share)]))
        copies = start_copies(pairs, sems)
        padded[:, :lead, :] = jnp.zeros((segments, lead, channels), F32)
        for copy in copies:
            copy.wait()
        both = product(gathered[...], weight[...])
        glu = both[:, :channels] * jax.nn.sigmoid(both[:, channels:])
        glu = glu.astype(BF16).astype(F32)
        padded[:, lead:, :] = glu.reshape(segments, LEN, channels)

        def segment(s, carry):
            result = jnp.zeros((LEN, channels), F32)
            for k in range(count):
                begin = lead - (count - 1) + k
                result = result + padded[s, begin : begin + LEN, :] * taps_ref[k : k + 1, :]
            conv_ref[aligned(s, LEN), :] = result
            return carry

        lax.fori_loop(0, segments, segment, 0)
        conv = conv_ref[...]
        ones = jnp.ones((8, channels), F32)
        over = (((1,), (1,)), ((), ()))
        for i, term in enumerate((conv, conv * conv)):
            sums_ref[8 * i : 8 * i + 8, :] = lax.dot_general(
                ones, term, over, precision=lax.Precision.HIGHEST, preferred_element_type=F32
            )

    return pl.pallas_call(
        run,
        in_specs=[SMEM, VMEM] + [HBM] * (nt + 1 + len(keys)),
        out_specs=[VMEM, VMEM],
        out_shape=[
            jax.ShapeDtypeStruct((total, channels), F32),
            jax.ShapeDtypeStruct((16, total), F32),
        ],
        scratch_shapes=[
            pltpu.VMEM((total, width), BF16),
            pltpu.VMEM((nf * depth, packed), BF16),
            pltpu.VMEM((segments, lead + LEN, channels), F32),
            pltpu.SemaphoreType.DMA((nt + 1 + len(keys),)),
        ],
        cost_estimate=pl.CostEstimate(
            flops=2 * total * width * packed,
            transcendentals=total * channels,
            bytes_accessed=2 * width * packed,
        ),
        compiler_params=pltpu.CompilerParams(vmem_limit_bytes=24 * MEBI),
        name="glu_conv",
    )(spot, taps, *[blocks[d] for d in range(nt)], own, *pieces.values())


def out_product(spot, sizes, conv, sums, gain, all_channels, own, pieces):
    ng, nf, nt = sizes
    total, channels = conv.shape
    rows = total // nt
    depth, cols = own.shape
    share = depth // ng
    keys = list(pieces)

    def run(spot_ref, conv_ref, gain_ref, *refs):
        sum_refs, refs = refs[: len(sums)], refs[len(sums) :]
        own_ref, refs = refs[0], refs[1:]
        piece_refs, refs = refs[: len(keys)], refs[len(keys) :]
        out_refs, refs = refs[:nt], refs[nt:]
        weight, mixed, sems = refs
        group, slab, member = spot_ref[0], spot_ref[1], spot_ref[2]
        pairs = [(own_ref, weight.at[slab])]
        for (d, e), ref in zip(keys, piece_refs):
            pairs.append((ref, weight.at[slab ^ d, aligned(group ^ e, share)]))
        copies = start_copies(pairs, sems)
        sums_all = sum(ref[...] for ref in sum_refs) * (1.0 / all_channels)
        row = lax.broadcasted_iota(jnp.int32, (total, total), 0)
        column = lax.broadcasted_iota(jnp.int32, (total, total), 1)

        def upright(line):
            return jnp.sum(jnp.where(row == column, line, 0.0), axis=1, keepdims=True)

        chan_mean = upright(sums_all[0:1, :])
        chan_var = upright(sums_all[8:9, :]) - chan_mean * chan_mean
        scaled = (conv_ref[...] - chan_mean) * lax.rsqrt(chan_var + chan_epsilon) * gain_ref[...]
        activated = (scaled * jax.nn.sigmoid(scaled)).astype(BF16)
        for copy in copies:
            copy.wait()
        for s in range(nf):
            mixed[:, s * cols : (s + 1) * cols] = product(activated, weight[s]).astype(BF16)
        targets = [(mixed.at[aligned(member ^ d, rows)], out_refs[d]) for d in range(nt)]
        for copy in start_copies(targets, sems):
            copy.wait()

    return pl.pallas_call(
        run,
        in_specs=[SMEM, VMEM, VMEM] + [VMEM] * len(sums) + [HBM] * (1 + len(keys)),
        out_specs=[HBM] * nt,
        out_shape=[jax.ShapeDtypeStruct((rows, nf * cols), BF16)] * nt,
        scratch_shapes=[
            pltpu.VMEM((nf, depth, cols), BF16),
            pltpu.VMEM((total, nf * cols), BF16),
            pltpu.SemaphoreType.DMA((max(nt, 1 + len(keys)),)),
        ],
        cost_estimate=pl.CostEstimate(
            flops=2 * total * channels * nf * cols,
            transcendentals=total * channels,
            bytes_accessed=2 * channels * nf * cols,
        ),
        compiler_params=pltpu.CompilerParams(vmem_limit_bytes=24 * MEBI),
        name="out_product",
    )(spot, conv, gain, *sums, own, *pieces.values())


def ffn_chunk(spot, sizes, blocks, up_own, up_pieces, taps, down_own, down_pieces):
    ng, nf, nt = sizes
    rows, width = blocks[0].shape
    total = nt * rows
    depth, packed = up_own.shape
    units, cols = down_own.shape
    up_share, down_share = depth // ng, units // ng
    whole = units // LANES * LANES
    rest = units - whole
    keys = list(up_pieces)
    wide = 2 * LANES

    def run(spot_ref, taps_ref, *refs):
        block_refs, refs = refs[:nt], refs[nt:]
        up_own_ref, down_own_ref, refs = refs[0], refs[1], refs[2:]
        up_refs, refs = refs[: len(keys)], refs[len(keys) :]
        down_refs, refs = refs[: len(keys)], refs[len(keys) :]
        out_refs, refs = refs[:nt], refs[nt:]
        gathered, up, down, hidden, mixed, sems = refs
        group, slab, member = spot_ref[0], spot_ref[1], spot_ref[2]
        pairs = [(block_refs[d], gathered.at[aligned(member ^ d, rows)]) for d in range(nt)]
        pairs.append((up_own_ref, up.at[aligned(slab, depth)]))
        for (d, e), ref in zip(keys, up_refs):
            place = (slab ^ d) * ng + (group ^ e)
            pairs.append((ref, up.at[aligned(place, up_share)]))
        copies = start_copies(pairs, sems)
        late = [(down_own_ref, down.at[slab])]
        for (d, e), ref in zip(keys, down_refs):
            late.append((ref, down.at[slab ^ d, aligned(group ^ e, down_share)]))
        late = start_copies(late, sems, len(pairs))
        for copy in copies:
            copy.wait()

        def conv(column, size):
            raw = product(gathered[...], up[:, column : column + size])
            raw = raw.astype(BF16).astype(F32)
            place = lax.broadcasted_iota(jnp.int32, raw.shape, 0) % LEN
            span = taps_ref.shape[0]
            result = raw * taps_ref[span - 1 : span, column : column + size]
            for back in range(1, span):
                moved = jnp.where(place >= back, pltpu.roll(raw, back, 0), 0.0)
                tap = taps_ref[span - 1 - back : span - back, column : column + size]
                result = result + moved * tap
            return result

        def gelu(v):
            return 0.5 * v * (1.0 + jnp.tanh((2.0 / jnp.pi) ** 0.5 * (v + 0.044715 * v * v * v)))

        for column in range(0, whole, wide):
            size = min(wide, whole - column)
            gate, val = conv(column, size), conv(whole + column, size)
            hidden[:, column : column + size] = (gelu(gate) * val).astype(BF16)
        if rest:
            both = conv(2 * whole, LANES)
            lane = lax.broadcasted_iota(jnp.int32, both.shape, 1)
            gated = gelu(both) * pltpu.roll(both, LANES - rest, 1)
            hidden[:, whole:] = jnp.where(lane < rest, gated, 0.0).astype(BF16)
        for copy in late:
            copy.wait()
        for s in range(nf):
            columns = slice(s * cols, (s + 1) * cols)
            mixed[:, columns] = product(hidden[:, :units], down[s]).astype(BF16)
        targets = [(mixed.at[aligned(member ^ d, rows)], out_refs[d]) for d in range(nt)]
        for copy in start_copies(targets, sems):
            copy.wait()

    flops = 2 * total * width * packed + 2 * total * units * nf * cols
    return pl.pallas_call(
        run,
        in_specs=[SMEM, VMEM] + [HBM] * (nt + 2 + 2 * len(keys)),
        out_specs=[HBM] * nt,
        out_shape=[jax.ShapeDtypeStruct((rows, nf * cols), BF16)] * nt,
        scratch_shapes=[
            pltpu.VMEM((total, width), BF16),
            pltpu.VMEM((nf * depth, packed), BF16),
            pltpu.VMEM((nf, units, cols), BF16),
            pltpu.VMEM((total, whole + (LANES if rest else 0)), BF16),
            pltpu.VMEM((total, nf * cols), BF16),
            pltpu.SemaphoreType.DMA((nt + 2 + 2 * len(keys),)),
        ],
        cost_estimate=pl.CostEstimate(
            flops=flops, transcendentals=total * units, bytes_accessed=2 * width * packed
        ),
        compiler_params=pltpu.CompilerParams(vmem_limit_bytes=24 * MEBI),
        name="ffn_chunk",
    )(
        spot,
        taps,
        *[blocks[d] for d in range(nt)],
        up_own,
        down_own,
        *up_pieces.values(),
        *down_pieces.values(),
    )


def pair_order(nf):
    return sorted(range(1, nf), key=lambda d: (d != 1, -d))


def exchange_shards(sizes):
    ng, nf, nt = sizes
    far = pair_order(nf)

    def shards(
        tokens,
        mix_gain,
        val_weight,
        gate_weight,
        conv_taps,
        chan_gain,
        out_weight,
        mix_post_gain,
        ffn_gain,
        up_gate_weight,
        up_val_weight,
        ffn_taps,
        down_weight,
        ffn_post_gain,
    ):
        group, slab, member = (lax.axis_index(a) for a in ("grp", "fs", "tp"))
        spot = jnp.stack([group, slab, member]).astype(jnp.int32)

        def fetch(piece_for):
            pieces = {}
            for d in far:
                pieces[d, 0] = swap(piece_for(d), "fs", nf, d)
            for d in far:
                for e in range(1, ng):
                    pieces[d, e] = swap(pieces[d, 0], "grp", ng, e)
            return pieces

        def share(array):
            return pick(array.reshape(ng, array.shape[0] // ng, array.shape[1]), group)

        local_ch = val_weight.shape[1]
        glu_own = jnp.concatenate([val_weight, gate_weight], axis=1)
        glu_share = jnp.concatenate([share(val_weight), share(gate_weight)], axis=1)
        glu_pieces = fetch(lambda d: glu_share)
        out_share = share(out_weight)
        out_pieces = fetch(lambda d: out_share)

        local_ff = up_gate_weight.shape[1]
        units = local_ff // nf
        whole = units // LANES * LANES

        def pack(gate, val):
            def block(s):
                a, b, c = s * units, s * units + whole, (s + 1) * units
                cut = [gate[..., a:b], val[..., a:b], gate[..., b:c], val[..., b:c]]
                return jnp.concatenate(cut, axis=-1)

            return jnp.stack([block(s) for s in range(nf)])

        up_blocks = pack(up_gate_weight, up_val_weight)
        up_own = pick(up_blocks, slab)
        up_halves = up_blocks.reshape(nf, ng, up_blocks.shape[1] // ng, 2 * units)
        up_pieces = fetch(lambda d: pick(up_halves, slab ^ d, group))
        down_own = pick(down_weight.reshape(nf, units, down_weight.shape[1]), slab)
        down_halves = down_weight.reshape(nf, ng, units // ng, down_weight.shape[1])
        down_pieces = fetch(lambda d: pick(down_halves, slab ^ d, group))
        own_taps = lax.dynamic_slice_in_dim(ffn_taps, member * local_ff, local_ff, 2)
        own_taps = pick(pack(own_taps[0], own_taps[1]), slab).astype(F32)

        def scaled(values, gain):
            mean = jnp.mean(values * values, axis=-1, keepdims=True)
            return values * lax.rsqrt(mean + norm_epsilon) * gain

        mix_taps = lax.dynamic_slice_in_dim(conv_taps, member * local_ch, local_ch, 1)
        own_gain = lax.dynamic_slice_in_dim(chan_gain[None], member * local_ch, local_ch, 1)
        (normed,) = row_kernel(lambda t, g: (scaled(t, g),), [tokens, mix_gain[None]], 1)
        row_blocks = gather_blocks(normed, "tp", nt)
        conv, sums = glu_conv(spot, sizes, row_blocks, glu_own, glu_pieces, mix_taps.astype(F32))
        all_sums = [sums] + [swap(sums, "tp", nt, d) for d in range(1, nt)]
        mixed = out_product(
            spot,
            sizes,
            conv,
            all_sums,
            own_gain.astype(F32),
            chan_gain.shape[0],
            out_weight,
            out_pieces,
        )
        terms = scatter_blocks(dict(enumerate(mixed)), "tp", nt)

        def residual_rows(t, post, gain, *parts):
            result = (t + scaled(sum(parts), post)).astype(BF16).astype(F32)
            return result, scaled(result, gain)

        residual, acted = row_kernel(
            residual_rows, [tokens, mix_post_gain[None], ffn_gain[None], *terms], 2
        )

        last = []
        for d in [0, *far]:
            block = swap(acted, "fs", nf, d) if d else acted
            blocks = gather_blocks(block, "tp", nt)
            parts = ffn_chunk(
                spot, sizes, blocks, up_own, up_pieces, own_taps, down_own, down_pieces
            )
            terms = scatter_blocks(dict(enumerate(parts)), "tp", nt)
            if d:
                terms = [swap(add_terms(terms), "fs", nf, d)]
            last += terms
        (result,) = row_kernel(
            lambda r, gain, *parts: (r + scaled(sum(parts), gain),),
            [residual, ffn_post_gain[None], *last],
            1,
        )
        return result

    return shards


def gather_shards(
    tokens,
    mix_gain,
    val_weight,
    gate_weight,
    conv_taps,
    chan_gain,
    out_weight,
    mix_post_gain,
    ffn_gain,
    up_gate_weight,
    up_val_weight,
    ffn_taps,
    down_weight,
    ffn_post_gain,
):
    member = lax.axis_index("tp")
    normed_own = rms_scale(tokens.astype(jnp.float32), mix_gain).astype(jnp.bfloat16)
    normed = lax.all_gather(normed_own, "tp", axis=0, tiled=True)
    local_ch = val_weight.shape[1]
    values = product(normed, lax.all_gather(val_weight, "fs", axis=0, tiled=True))
    gate_sums = product(normed, lax.all_gather(gate_weight, "fs", axis=0, tiled=True))
    glu_out = (values * jax.nn.sigmoid(gate_sums)).astype(jnp.bfloat16)
    own_taps = lax.dynamic_slice_in_dim(conv_taps, member * local_ch, local_ch, 1)
    conv_out = depthwise(glu_out, own_taps)
    totals, squares = lax.psum(
        (jnp.sum(conv_out, axis=1), jnp.sum(conv_out * conv_out, axis=1)), "tp"
    )
    all_channels = chan_gain.shape[0]
    chan_mean = totals[:, None] / all_channels
    chan_var = squares[:, None] / all_channels - chan_mean * chan_mean
    own_gain = lax.dynamic_slice_in_dim(chan_gain, member * local_ch, local_ch, 0)
    scaled = (conv_out - chan_mean) * lax.rsqrt(chan_var + chan_epsilon)
    activated = jax.nn.silu(scaled * own_gain.astype(jnp.float32)).astype(jnp.bfloat16)
    out_full = lax.all_gather(out_weight, "fs", axis=1, tiled=True)
    mixed_sum = lax.psum_scatter(
        product(activated, out_full).astype(jnp.bfloat16), "tp", scatter_dimension=0, tiled=True
    ).astype(jnp.float32)
    residual = tokens.astype(jnp.float32) + rms_scale(mixed_sum, mix_post_gain)
    residual = residual.astype(jnp.bfloat16)
    normed_share = rms_scale(residual.astype(jnp.float32), ffn_gain).astype(jnp.bfloat16)
    normed_ffn = lax.all_gather(normed_share, "tp", axis=0, tiled=True)
    local_ff = up_gate_weight.shape[1]
    own_ffn_taps = lax.dynamic_slice_in_dim(ffn_taps, member * local_ff, local_ff, 2)
    gate_full = lax.all_gather(up_gate_weight, "fs", axis=0, tiled=True)
    val_full = lax.all_gather(up_val_weight, "fs", axis=0, tiled=True)
    up_gate = product(normed_ffn, gate_full).astype(jnp.bfloat16)
    up_val = product(normed_ffn, val_full).astype(jnp.bfloat16)
    gate_conv = depthwise(up_gate, own_ffn_taps[0])
    val_conv = depthwise(up_val, own_ffn_taps[1])
    hidden = (jax.nn.gelu(gate_conv, approximate=True) * val_conv).astype(jnp.bfloat16)
    down_full = lax.all_gather(down_weight, "fs", axis=1, tiled=True)
    ffn_sum = lax.psum_scatter(
        product(hidden, down_full).astype(jnp.bfloat16), "tp", scatter_dimension=0, tiled=True
    ).astype(jnp.float32)
    return (residual.astype(jnp.float32) + rms_scale(ffn_sum, ffn_post_gain)).astype(jnp.bfloat16)


def solution(mesh):
    sizes = tuple(mesh.shape[a] for a in ("grp", "fs", "tp"))
    specs = (
        P(("grp", "fs", "tp"), None),
        P(),
        P("fs", "tp"),
        P("fs", "tp"),
        P(),
        P(),
        P("tp", "fs"),
        P(),
        P(),
        P("fs", "tp"),
        P("fs", "tp"),
        P(),
        P("tp", "fs"),
        P(),
    )
    powers = all(size & (size - 1) == 0 for size in sizes)
    exchange = powers and sizes[1] * sizes[2] <= 16

    def run(*args):
        units = args[9].shape[1] // (sizes[1] * sizes[2])
        cuts = units % LANES in (0, LANES // 2) and units % (16 * sizes[0]) == 0
        shards = exchange_shards(sizes) if exchange and cuts else gather_shards
        return jax.shard_map(
            shards,
            mesh=mesh,
            in_specs=specs,
            out_specs=P(("grp", "fs", "tp"), None),
            check_vma=False,
        )(*args)

    return run
```

```python
import jax
import jax.numpy as jnp
from jax import lax
from jax.experimental import pallas as pl
from jax.experimental.pallas import tpu as pltpu
from jax.sharding import PartitionSpec as P

LEN = 64
LANES = 128
BF16 = jnp.bfloat16
F32 = jnp.float32
MEBI = 2**20

norm_epsilon = 1e-06
chan_epsilon = 1e-05


def rms_scale(values, gain):
    inverse = lax.rsqrt(jnp.mean(values * values, axis=-1, keepdims=True) + norm_epsilon)
    return values * inverse * gain.astype(jnp.float32)


def depthwise(signal, tap_table):
    taps_count = tap_table.shape[0]
    channels = signal.shape[1]
    shaped = signal.astype(jnp.float32).reshape(signal.shape[0] // LEN, LEN, channels)
    padded = jnp.pad(shaped, ((0, 0), (taps_count - 1, 0), (0, 0)))
    tap_values = tap_table.astype(jnp.float32)
    result = jnp.zeros(shaped.shape, jnp.float32)
    for offset in range(taps_count):
        result = result + padded[:, offset : offset + LEN, :] * tap_values[offset]
    return result.reshape(signal.shape[0], channels)


def product(left, weight):
    return jnp.dot(left, weight, preferred_element_type=jnp.float32)


def swap(array, axis, size, bits):
    return lax.ppermute(array, axis, [(i, i ^ bits) for i in range(size)])


def halvings(size):
    return [1 << b for b in reversed(range(size.bit_length() - 1))]


def gather_blocks(block, axis, size):
    blocks = {0: block}
    for bits in halvings(size):
        for d in list(blocks):
            blocks[d | bits] = swap(blocks[d], axis, size, bits)
    return blocks


def scatter_blocks(blocks, axis, size):
    terms = {d: [b] for d, b in blocks.items()}
    for bits in reversed(halvings(size)):
        kept = {}
        for d in terms:
            if not d & bits:
                sent = add_terms(terms[d | bits])
                other = swap(sent, axis, size, bits)
                kept[d] = [*terms[d], other]
        terms = kept
    return terms[0]


def add_terms(terms):
    if len(terms) == 1:
        return terms[0]
    return sum(t.astype(F32) for t in terms).astype(BF16)


VMEM = pl.BlockSpec(memory_space=pltpu.VMEM)
SMEM = pl.BlockSpec(memory_space=pltpu.SMEM)
ANY = pl.BlockSpec(memory_space=pl.ANY)
HBM = pl.BlockSpec(memory_space=pltpu.HBM)


def aligned(index, size):
    return pl.ds(pl.multiple_of(index * size, 16), size)


def start_copies(pairs, sems, first=0):
    copies = []
    for i, (source, target) in enumerate(pairs):
        copies.append(pltpu.make_async_copy(source, target, sems.at[first + i]))
        copies[-1].start()
    return copies


def row_kernel(body, arrays, outs):
    count = len(arrays)

    def run(*refs):
        results = body(*[ref[...].astype(F32) for ref in refs[:count]])
        for ref, result in zip(refs[count:], results):
            ref[...] = result.astype(ref.dtype)

    return pl.pallas_call(
        run,
        in_specs=[VMEM] * count,
        out_specs=[VMEM] * outs,
        out_shape=[jax.ShapeDtypeStruct(arrays[0].shape, BF16)] * outs,
        cost_estimate=pl.CostEstimate(
            flops=8 * arrays[0].size, transcendentals=0, bytes_accessed=4 * arrays[0].size
        ),
        compiler_params=pltpu.CompilerParams(vmem_limit_bytes=12 * MEBI),
    )(*arrays)


def glu_conv(spot, sizes, blocks, val, gate, pieces, taps):
    ng, nf, nt = sizes
    rows, width = blocks[0].shape
    total = nt * rows
    depth, channels = val.shape
    packed = 2 * channels
    share = depth // ng
    count = taps.shape[0]
    lead = -(-(count - 1) // 8) * 8
    segments = total // LEN
    keys = list(pieces)

    def run(spot_ref, taps_ref, *refs):
        block_refs, refs = refs[:nt], refs[nt:]
        own_refs, refs = refs[:2], refs[2:]
        piece_refs, refs = refs[: len(keys)], refs[len(keys) :]
        conv_ref, sums_ref, gathered, weight, padded, sems = refs
        group, slab, member = spot_ref[0], spot_ref[1], spot_ref[2]
        pairs = [(block_refs[d], gathered.at[aligned(member ^ d, rows)]) for d in range(nt)]
        for i, ref in enumerate(own_refs):
            columns = pl.ds(i * channels, channels)
            pairs.append((ref, weight.at[aligned(slab, depth), columns]))
        for (d, e), ref in zip(keys, piece_refs):
            place = (slab ^ d) * ng + (group ^ e)
            pairs.append((ref, weight.at[aligned(place, share)]))
        copies = start_copies(pairs, sems)
        padded[:, :lead, :] = jnp.zeros((segments, lead, channels), F32)
        for copy in copies:
            copy.wait()
        both = product(gathered[...], weight[...])
        glu = both[:, :channels] * jax.nn.sigmoid(both[:, channels:])
        glu = glu.astype(BF16).astype(F32)
        padded[:, lead:, :] = glu.reshape(segments, LEN, channels)

        def segment(s, carry):
            result = jnp.zeros((LEN, channels), F32)
            for k in range(count):
                begin = lead - (count - 1) + k
                result = result + padded[s, begin : begin + LEN, :] * taps_ref[k : k + 1, :]
            conv_ref[aligned(s, LEN), :] = result
            return carry

        lax.fori_loop(0, segments, segment, 0)
        conv = conv_ref[...]
        ones = jnp.ones((8, channels), F32)
        over = (((1,), (1,)), ((), ()))
        for i, term in enumerate((conv, conv * conv)):
            sums_ref[8 * i : 8 * i + 8, :] = lax.dot_general(
                ones, term, over, precision=lax.Precision.HIGHEST, preferred_element_type=F32
            )

    return pl.pallas_call(
        run,
        in_specs=[SMEM, VMEM] + [ANY] * nt + [HBM] * 2 + [ANY] * len(keys),
        out_specs=[VMEM, VMEM],
        out_shape=[
            jax.ShapeDtypeStruct((total, channels), F32),
            jax.ShapeDtypeStruct((16, total), F32),
        ],
        scratch_shapes=[
            pltpu.VMEM((total, width), BF16),
            pltpu.VMEM((nf * depth, packed), BF16),
            pltpu.VMEM((segments, lead + LEN, channels), F32),
            pltpu.SemaphoreType.DMA((nt + 2 + len(keys),)),
        ],
        cost_estimate=pl.CostEstimate(
            flops=2 * total * width * packed,
            transcendentals=total * channels,
            bytes_accessed=2 * width * packed,
        ),
        compiler_params=pltpu.CompilerParams(vmem_limit_bytes=24 * MEBI),
        name="glu_conv",
    )(spot, taps, *[blocks[d] for d in range(nt)], val, gate, *pieces.values())


def out_product(spot, sizes, conv, sums, gain, all_channels, own, pieces):
    ng, nf, nt = sizes
    total, channels = conv.shape
    rows = total // nt
    depth, cols = own.shape
    share = depth // ng
    keys = list(pieces)

    def run(spot_ref, conv_ref, gain_ref, *refs):
        sum_refs, refs = refs[: len(sums)], refs[len(sums) :]
        own_ref, refs = refs[0], refs[1:]
        piece_refs, refs = refs[: len(keys)], refs[len(keys) :]
        out_refs, refs = refs[:nt], refs[nt:]
        weight, mixed, sems = refs
        group, slab, member = spot_ref[0], spot_ref[1], spot_ref[2]
        pairs = [(own_ref, weight.at[slab])]
        for (d, e), ref in zip(keys, piece_refs):
            pairs.append((ref, weight.at[slab ^ d, aligned(group ^ e, share)]))
        copies = start_copies(pairs, sems)
        sums_all = sum(ref[...] for ref in sum_refs) * (1.0 / all_channels)
        row = lax.broadcasted_iota(jnp.int32, (total, total), 0)
        column = lax.broadcasted_iota(jnp.int32, (total, total), 1)

        def upright(line):
            return jnp.sum(jnp.where(row == column, line, 0.0), axis=1, keepdims=True)

        chan_mean = upright(sums_all[0:1, :])
        chan_var = upright(sums_all[8:9, :]) - chan_mean * chan_mean
        scaled = (conv_ref[...] - chan_mean) * lax.rsqrt(chan_var + chan_epsilon) * gain_ref[...]
        activated = (scaled * jax.nn.sigmoid(scaled)).astype(BF16)
        for copy in copies:
            copy.wait()
        for s in range(nf):
            mixed[:, s * cols : (s + 1) * cols] = product(activated, weight[s]).astype(BF16)
        targets = [(mixed.at[aligned(member ^ d, rows)], out_refs[d]) for d in range(nt)]
        for copy in start_copies(targets, sems):
            copy.wait()

    return pl.pallas_call(
        run,
        in_specs=[SMEM, VMEM, VMEM] + [VMEM] * len(sums) + [HBM] + [ANY] * len(keys),
        out_specs=[ANY] * nt,
        out_shape=[jax.ShapeDtypeStruct((rows, nf * cols), BF16)] * nt,
        scratch_shapes=[
            pltpu.VMEM((nf, depth, cols), BF16),
            pltpu.VMEM((total, nf * cols), BF16),
            pltpu.SemaphoreType.DMA((max(nt, 1 + len(keys)),)),
        ],
        cost_estimate=pl.CostEstimate(
            flops=2 * total * channels * nf * cols,
            transcendentals=total * channels,
            bytes_accessed=2 * channels * nf * cols,
        ),
        compiler_params=pltpu.CompilerParams(vmem_limit_bytes=24 * MEBI),
        name="out_product",
    )(spot, conv, gain, *sums, own, *pieces.values())


def mix_shares(spot, sizes, val, gate, out):
    ng = sizes[0]
    depth, channels = val.shape
    tall, cols = out.shape

    def run(spot_ref, val_ref, gate_ref, out_ref, glu_share, out_share, glu_held, out_held, sems):
        group = spot_ref[0]
        rows = aligned(group, depth // ng)
        pairs = [
            (val_ref.at[rows], glu_held.at[:, pl.ds(0, channels)]),
            (gate_ref.at[rows], glu_held.at[:, pl.ds(channels, channels)]),
            (out_ref.at[aligned(group, tall // ng)], out_held),
        ]
        copies = start_copies(pairs, sems)
        for copy in copies[:2]:
            copy.wait()
        outward = start_copies([(glu_held, glu_share)], sems, 3)
        copies[2].wait()
        outward += start_copies([(out_held, out_share)], sems, 4)
        for copy in outward:
            copy.wait()

    return pl.pallas_call(
        run,
        in_specs=[SMEM, HBM, HBM, HBM],
        out_specs=[ANY, ANY],
        out_shape=[
            jax.ShapeDtypeStruct((depth // ng, 2 * channels), BF16),
            jax.ShapeDtypeStruct((tall // ng, cols), BF16),
        ],
        scratch_shapes=[
            pltpu.VMEM((depth // ng, 2 * channels), BF16),
            pltpu.VMEM((tall // ng, cols), BF16),
            pltpu.SemaphoreType.DMA((5,)),
        ],
        compiler_params=pltpu.CompilerParams(vmem_limit_bytes=60 * MEBI),
        name="mix_shares",
    )(spot, val, gate, out)


def ffn_shares(spot, sizes, gate, val, down):
    ng, nf, _ = sizes
    depth, local_ff = gate.shape
    cols = down.shape[1]
    units = local_ff // nf
    whole = units // LANES * LANES
    rest = units - whole
    share = depth // ng
    packed = 2 * units
    count = nf - 1
    tall = (whole // ng, rest // ng)

    def run(spot_ref, *refs):
        sources, refs = refs[:3], refs[3:]
        up_refs, refs = refs[:count], refs[count:]
        down_refs, refs = refs[:count], refs[count:]
        up_own_ref, down_own_ref, gate_ref, val_ref, down_ref, halves, sems = refs
        group, slab = spot_ref[0], spot_ref[1]
        rows = aligned(group, share)
        for copy in start_copies(zip(sources, (gate_ref, val_ref, down_ref)), sems):
            copy.wait()
        mine = pl.ds(pl.multiple_of(slab * whole, LANES), whole)
        pairs = [
            (gate_ref.at[:, mine], up_own_ref.at[:, pl.ds(0, whole)]),
            (val_ref.at[:, mine], up_own_ref.at[:, pl.ds(whole, whole)]),
            (down_ref.at[mine], down_own_ref.at[pl.ds(0, whole)]),
        ]
        if rest:
            last = pl.ds(pl.multiple_of(nf * whole + slab * rest, 16), rest)
            pairs.append((down_ref.at[last], down_own_ref.at[pl.ds(whole, rest)]))
        for d in range(1, nf):
            there = slab ^ d
            columns = pl.ds(pl.multiple_of(there * whole, LANES), whole)
            for i, ref in enumerate((gate_ref, val_ref)):
                pairs.append((ref.at[rows, columns], up_refs[d - 1].at[:, pl.ds(i * whole, whole)]))
            first = pl.multiple_of(there * whole + group * tall[0], 16)
            pairs.append(
                (down_ref.at[pl.ds(first, tall[0])], down_refs[d - 1].at[pl.ds(0, tall[0])])
            )
            if rest:
                first = pl.multiple_of(nf * whole + there * rest + group * tall[1], 16)
                part = down_refs[d - 1].at[pl.ds(tall[0], tall[1])]
                pairs.append((down_ref.at[pl.ds(first, tall[1])], part))
        copies = start_copies(pairs, sems, 3)
        if rest:
            lane = lax.broadcasted_iota(jnp.int32, (depth, LANES), 1)
            for s in range(nf):
                begin = nf * whole + s * rest // LANES * LANES
                pair = [ref[:, begin : begin + LANES].astype(F32) for ref in (gate_ref, val_ref)]
                moved = 1 if s * rest % LANES == 0 else 0
                pair[moved] = pltpu.roll(pair[moved], rest, 1)
                halves[s] = jnp.where(lane < rest, pair[0], pair[1]).astype(BF16)
            pairs = [
                (halves.at[slab ^ d, rows], up_refs[d - 1].at[:, pl.ds(2 * whole, LANES)])
                for d in range(1, nf)
            ]
            pairs.append((halves.at[slab], up_own_ref.at[:, pl.ds(2 * whole, LANES)]))
            copies += start_copies(pairs, sems, 3 + len(copies))
        for copy in copies:
            copy.wait()

    outs = pl.pallas_call(
        run,
        in_specs=[SMEM, HBM, HBM, HBM],
        out_specs=[ANY] * (2 * count + 2),
        out_shape=[jax.ShapeDtypeStruct((share, packed), BF16)] * count
        + [jax.ShapeDtypeStruct((units // ng, cols), BF16)] * count
        + [jax.ShapeDtypeStruct((depth, packed), BF16)]
        + [jax.ShapeDtypeStruct((units, cols), BF16)],
        scratch_shapes=[
            pltpu.VMEM(gate.shape, BF16),
            pltpu.VMEM(val.shape, BF16),
            pltpu.VMEM(down.shape, BF16),
            pltpu.VMEM((nf, depth, LANES), BF16),
            pltpu.SemaphoreType.DMA((8 + 5 * count,)),
        ],
        cost_estimate=pl.CostEstimate(
            flops=depth * packed, transcendentals=0, bytes_accessed=8 * depth * packed
        ),
        compiler_params=pltpu.CompilerParams(vmem_limit_bytes=60 * MEBI),
        name="ffn_shares",
    )(spot, gate, val, down)
    ups = {d: outs[d - 1] for d in range(1, nf)}
    downs = {d: outs[count + d - 1] for d in range(1, nf)}
    return ups, downs, outs[-2], outs[-1]


def ffn_weights(spot, sizes, up_own, up_pieces, down_own, down_pieces):
    ng, nf, _ = sizes
    depth, packed = up_own.shape
    units, cols = down_own.shape
    whole = units // LANES * LANES
    rest = units - whole
    padded = -(-units // LANES) * LANES
    share = depth // ng
    tall = (whole // ng, rest // ng)
    keys = list(up_pieces)

    def run(spot_ref, up_own_ref, down_own_ref, *refs):
        up_refs, refs = refs[: len(keys)], refs[len(keys) :]
        down_refs, refs = refs[: len(keys)], refs[len(keys) :]
        up, down, sems = refs
        group, slab = spot_ref[0], spot_ref[1]
        pairs = [
            (up_own_ref, up.at[aligned(slab, depth)]),
            (down_own_ref, down.at[slab, pl.ds(0, units)]),
        ]
        for (d, e), up_ref, down_ref in zip(keys, up_refs, down_refs):
            place = (slab ^ d) * ng + (group ^ e)
            pairs.append((up_ref, up.at[aligned(place, share)]))
            target = down.at[slab ^ d, aligned(group ^ e, tall[0])]
            pairs.append((down_ref.at[pl.ds(0, tall[0])], target))
            if rest:
                first = pl.multiple_of(whole + (group ^ e) * tall[1], 16)
                target = down.at[slab ^ d, pl.ds(first, tall[1])]
                pairs.append((down_ref.at[pl.ds(tall[0], tall[1])], target))
        copies = start_copies(pairs, sems)
        if padded > units:
            down[:, units:, :] = jnp.zeros((nf, padded - units, cols), BF16)
        for copy in copies:
            copy.wait()

    return pl.pallas_call(
        run,
        in_specs=[SMEM] + [ANY] * (2 + 2 * len(keys)),
        out_specs=[VMEM, VMEM],
        out_shape=[
            jax.ShapeDtypeStruct((nf * depth, packed), BF16),
            jax.ShapeDtypeStruct((nf, padded, cols), BF16),
        ],
        scratch_shapes=[pltpu.SemaphoreType.DMA((2 + 3 * len(keys),))],
        cost_estimate=pl.CostEstimate(
            flops=nf * depth * packed, transcendentals=0, bytes_accessed=4 * nf * depth * packed
        ),
        compiler_params=pltpu.CompilerParams(vmem_limit_bytes=12 * MEBI),
        name="ffn_weights",
    )(spot, up_own, down_own, *up_pieces.values(), *down_pieces.values())


def ffn_chunk(spot, sizes, blocks, up, taps, down):
    nt = sizes[2]
    rows, width = blocks[0].shape
    total = nt * rows
    packed = up.shape[1]
    parts, padded, cols = down.shape
    units = packed // 2
    whole = units // LANES * LANES
    rest = units - whole
    wide = 2 * LANES

    def run(spot_ref, taps_ref, up, down, *refs):
        block_refs, refs = refs[:nt], refs[nt:]
        out_refs, refs = refs[:nt], refs[nt:]
        gathered, hidden, mixed, sems = refs
        member = spot_ref[2]
        pairs = [(block_refs[d], gathered.at[aligned(member ^ d, rows)]) for d in range(nt)]
        for copy in start_copies(pairs, sems):
            copy.wait()

        def conv(column, size):
            raw = product(gathered[...], up[:, column : column + size])
            raw = raw.astype(BF16).astype(F32)
            place = lax.broadcasted_iota(jnp.int32, raw.shape, 0) % LEN
            span = taps_ref.shape[0]
            result = raw * taps_ref[span - 1 : span, column : column + size]
            for back in range(1, span):
                moved = jnp.where(place >= back, pltpu.roll(raw, back, 0), 0.0)
                tap = taps_ref[span - 1 - back : span - back, column : column + size]
                result = result + moved * tap
            return result

        def gelu(v):
            return 0.5 * v * (1.0 + jnp.tanh((2.0 / jnp.pi) ** 0.5 * (v + 0.044715 * v * v * v)))

        for column in range(0, whole, wide):
            size = min(wide, whole - column)
            gate, val = conv(column, size), conv(whole + column, size)
            hidden[:, column : column + size] = (gelu(gate) * val).astype(BF16)
        if rest:
            both = conv(2 * whole, LANES)
            lane = lax.broadcasted_iota(jnp.int32, both.shape, 1)
            gated = gelu(both) * pltpu.roll(both, LANES - rest, 1)
            hidden[:, whole:] = jnp.where(lane < rest, gated, 0.0).astype(BF16)
        outward = []
        for s in range(parts):
            columns = pl.ds(s * cols, cols)
            mixed[:, columns] = product(hidden[...], down[s]).astype(BF16)
            targets = [
                (mixed.at[aligned(member ^ d, rows), columns], out_refs[d].at[:, columns])
                for d in range(nt)
            ]
            outward += start_copies(targets, sems, nt + len(outward))
        for copy in outward:
            copy.wait()

    flops = 2 * total * width * packed + 2 * total * units * parts * cols
    return pl.pallas_call(
        run,
        in_specs=[SMEM, VMEM, VMEM, VMEM] + [ANY] * nt,
        out_specs=[ANY] * nt,
        out_shape=[jax.ShapeDtypeStruct((rows, parts * cols), BF16)] * nt,
        scratch_shapes=[
            pltpu.VMEM((total, width), BF16),
            pltpu.VMEM((total, padded), BF16),
            pltpu.VMEM((total, parts * cols), BF16),
            pltpu.SemaphoreType.DMA((nt + nt * parts,)),
        ],
        cost_estimate=pl.CostEstimate(
            flops=flops, transcendentals=total * units, bytes_accessed=2 * width * packed
        ),
        compiler_params=pltpu.CompilerParams(vmem_limit_bytes=20 * MEBI),
        name="ffn_chunk",
    )(spot, taps, up, down, *[blocks[d] for d in range(nt)])


def exchange_shards(sizes):
    ng, nf, nt = sizes

    def shards(
        tokens,
        mix_gain,
        val_weight,
        gate_weight,
        conv_taps,
        chan_gain,
        out_weight,
        mix_post_gain,
        ffn_gain,
        up_gate_weight,
        up_val_weight,
        ffn_taps,
        down_weight,
        ffn_post_gain,
    ):
        group, slab, member = (lax.axis_index(a) for a in ("grp", "fs", "tp"))
        spot = jnp.stack([group, slab, member]).astype(jnp.int32)

        def share_out(blocks):
            pieces = {(d, 0): blocks[d] for d in range(1, nf)}
            for d in range(1, nf):
                for e in range(1, ng):
                    pieces[d, e] = swap(blocks[d], "grp", ng, e)
            return pieces

        def fetch(shares):
            sent = {d: swap(shares[d], "fs", nf, d) for d in shares}
            return share_out(sent)

        def fetch_all(mine):
            return share_out(gather_blocks(mine, "fs", nf))

        local_ch = val_weight.shape[1]
        glu_share, out_share = mix_shares(spot, sizes, val_weight, gate_weight, out_weight)
        glu_pieces = fetch_all(glu_share)
        out_pieces = fetch_all(out_share)

        local_ff = up_gate_weight.shape[1]
        units = local_ff // nf
        whole = units // LANES * LANES
        rest = units - whole
        up_shares, down_shares, up_own, down_own = ffn_shares(
            spot, sizes, up_gate_weight, up_val_weight, down_weight
        )
        up_pieces, down_pieces = fetch(up_shares), fetch(down_shares)
        up_full, down_full = ffn_weights(spot, sizes, up_own, up_pieces, down_own, down_pieces)
        begin = member * local_ff
        taps_whole = lax.dynamic_slice_in_dim(ffn_taps, begin + slab * whole, whole, 2)
        own_taps = [taps_whole[0], taps_whole[1]]
        if rest:
            first = begin + nf * whole + slab * rest
            taps_rest = lax.dynamic_slice_in_dim(ffn_taps, first, rest, 2)
            own_taps += [taps_rest[0], taps_rest[1]]
        own_taps = jnp.concatenate(own_taps, axis=1).astype(F32)

        def scaled(values, gain):
            mean = jnp.mean(values * values, axis=-1, keepdims=True)
            return values * lax.rsqrt(mean + norm_epsilon) * gain

        mix_taps = lax.dynamic_slice_in_dim(conv_taps, member * local_ch, local_ch, 1)
        own_gain = lax.dynamic_slice_in_dim(chan_gain[None], member * local_ch, local_ch, 1)
        (normed,) = row_kernel(lambda t, g: (scaled(t, g),), [tokens, mix_gain[None]], 1)
        row_blocks = gather_blocks(normed, "tp", nt)
        conv, sums = glu_conv(
            spot, sizes, row_blocks, val_weight, gate_weight, glu_pieces, mix_taps.astype(F32)
        )
        all_sums = [sums] + [swap(sums, "tp", nt, d) for d in range(1, nt)]
        mixed = out_product(
            spot,
            sizes,
            conv,
            all_sums,
            own_gain.astype(F32),
            chan_gain.shape[0],
            out_weight,
            out_pieces,
        )
        terms = scatter_blocks(dict(enumerate(mixed)), "tp", nt)

        def residual_rows(t, post, gain, *parts):
            result = (t + scaled(sum(parts), post)).astype(BF16).astype(F32)
            return result, scaled(result, gain)

        residual, acted = row_kernel(
            residual_rows, [tokens, mix_post_gain[None], ffn_gain[None], *terms], 2
        )

        last = []
        acts = gather_blocks(acted, "fs", nf)
        for d in range(nf):
            blocks = gather_blocks(acts[d], "tp", nt)
            parts = ffn_chunk(spot, sizes, blocks, up_full, own_taps, down_full)
            terms = scatter_blocks(dict(enumerate(parts)), "tp", nt)
            if d:
                terms = [swap(add_terms(terms), "fs", nf, d)]
            last += terms
        (result,) = row_kernel(
            lambda r, gain, *parts: (r + scaled(sum(parts), gain),),
            [residual, ffn_post_gain[None], *last],
            1,
        )
        return result

    return shards


def gather_shards(
    tokens,
    mix_gain,
    val_weight,
    gate_weight,
    conv_taps,
    chan_gain,
    out_weight,
    mix_post_gain,
    ffn_gain,
    up_gate_weight,
    up_val_weight,
    ffn_taps,
    down_weight,
    ffn_post_gain,
):
    member = lax.axis_index("tp")
    normed_own = rms_scale(tokens.astype(jnp.float32), mix_gain).astype(jnp.bfloat16)
    normed = lax.all_gather(normed_own, "tp", axis=0, tiled=True)
    local_ch = val_weight.shape[1]
    values = product(normed, lax.all_gather(val_weight, "fs", axis=0, tiled=True))
    gate_sums = product(normed, lax.all_gather(gate_weight, "fs", axis=0, tiled=True))
    glu_out = (values * jax.nn.sigmoid(gate_sums)).astype(jnp.bfloat16)
    own_taps = lax.dynamic_slice_in_dim(conv_taps, member * local_ch, local_ch, 1)
    conv_out = depthwise(glu_out, own_taps)
    totals, squares = lax.psum(
        (jnp.sum(conv_out, axis=1), jnp.sum(conv_out * conv_out, axis=1)), "tp"
    )
    all_channels = chan_gain.shape[0]
    chan_mean = totals[:, None] / all_channels
    chan_var = squares[:, None] / all_channels - chan_mean * chan_mean
    own_gain = lax.dynamic_slice_in_dim(chan_gain, member * local_ch, local_ch, 0)
    scaled = (conv_out - chan_mean) * lax.rsqrt(chan_var + chan_epsilon)
    activated = jax.nn.silu(scaled * own_gain.astype(jnp.float32)).astype(jnp.bfloat16)
    out_full = lax.all_gather(out_weight, "fs", axis=1, tiled=True)
    mixed_sum = lax.psum_scatter(
        product(activated, out_full).astype(jnp.bfloat16), "tp", scatter_dimension=0, tiled=True
    ).astype(jnp.float32)
    residual = tokens.astype(jnp.float32) + rms_scale(mixed_sum, mix_post_gain)
    residual = residual.astype(jnp.bfloat16)
    normed_share = rms_scale(residual.astype(jnp.float32), ffn_gain).astype(jnp.bfloat16)
    normed_ffn = lax.all_gather(normed_share, "tp", axis=0, tiled=True)
    local_ff = up_gate_weight.shape[1]
    own_ffn_taps = lax.dynamic_slice_in_dim(ffn_taps, member * local_ff, local_ff, 2)
    gate_full = lax.all_gather(up_gate_weight, "fs", axis=0, tiled=True)
    val_full = lax.all_gather(up_val_weight, "fs", axis=0, tiled=True)
    up_gate = product(normed_ffn, gate_full).astype(jnp.bfloat16)
    up_val = product(normed_ffn, val_full).astype(jnp.bfloat16)
    gate_conv = depthwise(up_gate, own_ffn_taps[0])
    val_conv = depthwise(up_val, own_ffn_taps[1])
    hidden = (jax.nn.gelu(gate_conv, approximate=True) * val_conv).astype(jnp.bfloat16)
    down_full = lax.all_gather(down_weight, "fs", axis=1, tiled=True)
    ffn_sum = lax.psum_scatter(
        product(hidden, down_full).astype(jnp.bfloat16), "tp", scatter_dimension=0, tiled=True
    ).astype(jnp.float32)
    return (residual.astype(jnp.float32) + rms_scale(ffn_sum, ffn_post_gain)).astype(jnp.bfloat16)


def solution(mesh):
    sizes = tuple(mesh.shape[a] for a in ("grp", "fs", "tp"))
    specs = (
        P(("grp", "fs", "tp"), None),
        P(),
        P("fs", "tp"),
        P("fs", "tp"),
        P(),
        P(),
        P("tp", "fs"),
        P(),
        P(),
        P("fs", "tp"),
        P("fs", "tp"),
        P(),
        P("tp", "fs"),
        P(),
    )
    powers = all(size & (size - 1) == 0 for size in sizes)
    exchange = powers and sizes[1] * sizes[2] <= 16

    def run(*args):
        units = args[9].shape[1] // (sizes[1] * sizes[2])
        cuts = units % LANES in (0, LANES // 2) and units % (32 * sizes[0]) == 0
        shards = exchange_shards(sizes) if exchange and cuts else gather_shards
        return jax.shard_map(
            shards,
            mesh=mesh,
            in_specs=specs,
            out_specs=P(("grp", "fs", "tp"), None),
            check_vma=False,
        )(*args)

    return run
```

```python
import jax
import jax.numpy as jnp
from jax import lax
from jax.experimental import pallas as pl
from jax.experimental.pallas import tpu as pltpu
from jax.sharding import PartitionSpec as P

LEN = 64
LANES = 128
BF16 = jnp.bfloat16
F32 = jnp.float32
MEBI = 2**20

norm_epsilon = 1e-06
chan_epsilon = 1e-05


def rms_scale(values, gain):
    inverse = lax.rsqrt(jnp.mean(values * values, axis=-1, keepdims=True) + norm_epsilon)
    return values * inverse * gain.astype(jnp.float32)


def depthwise(signal, tap_table):
    taps_count = tap_table.shape[0]
    channels = signal.shape[1]
    shaped = signal.astype(jnp.float32).reshape(signal.shape[0] // LEN, LEN, channels)
    padded = jnp.pad(shaped, ((0, 0), (taps_count - 1, 0), (0, 0)))
    tap_values = tap_table.astype(jnp.float32)
    result = jnp.zeros(shaped.shape, jnp.float32)
    for offset in range(taps_count):
        result = result + padded[:, offset : offset + LEN, :] * tap_values[offset]
    return result.reshape(signal.shape[0], channels)


def product(left, weight):
    return jnp.dot(left, weight, preferred_element_type=jnp.float32)


def swap(array, axis, size, bits):
    return lax.ppermute(array, axis, [(i, i ^ bits) for i in range(size)])


def halvings(size):
    return [1 << b for b in reversed(range(size.bit_length() - 1))]


def gather_blocks(block, axis, size):
    blocks = {0: block}
    for bits in halvings(size):
        for d in list(blocks):
            blocks[d | bits] = swap(blocks[d], axis, size, bits)
    return blocks


def scatter_blocks(blocks, axis, size):
    terms = {d: [b] for d, b in blocks.items()}
    for bits in reversed(halvings(size)):
        kept = {}
        for d in terms:
            if not d & bits:
                sent = add_terms(terms[d | bits])
                other = swap(sent, axis, size, bits)
                kept[d] = [*terms[d], other]
        terms = kept
    return terms[0]


def add_terms(terms):
    if len(terms) == 1:
        return terms[0]
    return sum(t.astype(F32) for t in terms).astype(BF16)


VMEM = pl.BlockSpec(memory_space=pltpu.VMEM)
SMEM = pl.BlockSpec(memory_space=pltpu.SMEM)
ANY = pl.BlockSpec(memory_space=pl.ANY)
HBM = pl.BlockSpec(memory_space=pltpu.HBM)


def aligned(index, size):
    return pl.ds(pl.multiple_of(index * size, 16), size)


def start_copies(pairs, sems, first=0):
    copies = []
    for i, (source, target) in enumerate(pairs):
        copies.append(pltpu.make_async_copy(source, target, sems.at[first + i]))
        copies[-1].start()
    return copies


def row_kernel(body, arrays, outs):
    count = len(arrays)

    def run(*refs):
        results = body(*[ref[...].astype(F32) for ref in refs[:count]])
        for ref, result in zip(refs[count:], results):
            ref[...] = result.astype(ref.dtype)

    return pl.pallas_call(
        run,
        in_specs=[VMEM] * count,
        out_specs=[VMEM] * outs,
        out_shape=[jax.ShapeDtypeStruct(arrays[0].shape, BF16)] * outs,
        cost_estimate=pl.CostEstimate(
            flops=8 * arrays[0].size, transcendentals=0, bytes_accessed=4 * arrays[0].size
        ),
        compiler_params=pltpu.CompilerParams(vmem_limit_bytes=12 * MEBI),
    )(*arrays)


def glu_conv(spot, sizes, blocks, val, gate, pieces, taps):
    _, nf, nt = sizes
    rows, width = blocks[0].shape
    total = nt * rows
    depth, channels = val.shape
    packed = 2 * channels
    count = taps.shape[0]
    lead = -(-(count - 1) // 8) * 8
    segments = total // LEN
    keys = list(pieces)

    def run(spot_ref, taps_ref, *refs):
        block_refs, refs = refs[:nt], refs[nt:]
        own_refs, refs = refs[:2], refs[2:]
        piece_refs, refs = refs[: len(keys)], refs[len(keys) :]
        conv_ref, sums_ref, gathered, weight, padded, sems = refs
        group, slab, member = spot_ref[0], spot_ref[1], spot_ref[2]
        pairs = [(block_refs[d], gathered.at[aligned(member ^ d, rows)]) for d in range(nt)]
        for i, ref in enumerate(own_refs):
            columns = pl.ds(i * channels, channels)
            pairs.append((ref, weight.at[aligned(slab, depth), columns]))
        for (d, e), ref in zip(keys, piece_refs):
            columns = pl.ds(pl.multiple_of((group ^ e) * channels, LANES), channels)
            pairs.append((ref, weight.at[aligned(slab ^ d, depth), columns]))
        copies = start_copies(pairs, sems)
        padded[:, :lead, :] = jnp.zeros((segments, lead, channels), F32)
        for copy in copies:
            copy.wait()
        both = product(gathered[...], weight[...])
        glu = both[:, :channels] * jax.nn.sigmoid(both[:, channels:])
        glu = glu.astype(BF16).astype(F32)
        padded[:, lead:, :] = glu.reshape(segments, LEN, channels)

        def segment(s, carry):
            result = jnp.zeros((LEN, channels), F32)
            for k in range(count):
                begin = lead - (count - 1) + k
                result = result + padded[s, begin : begin + LEN, :] * taps_ref[k : k + 1, :]
            conv_ref[aligned(s, LEN), :] = result
            return carry

        lax.fori_loop(0, segments, segment, 0)
        conv = conv_ref[...]
        ones = jnp.ones((8, channels), F32)
        over = (((1,), (1,)), ((), ()))
        for i, term in enumerate((conv, conv * conv)):
            sums_ref[8 * i : 8 * i + 8, :] = lax.dot_general(
                ones, term, over, precision=lax.Precision.HIGHEST, preferred_element_type=F32
            )

    return pl.pallas_call(
        run,
        in_specs=[SMEM, VMEM] + [ANY] * nt + [HBM] * 2 + [ANY] * len(keys),
        out_specs=[VMEM, VMEM],
        out_shape=[
            jax.ShapeDtypeStruct((total, channels), F32),
            jax.ShapeDtypeStruct((16, total), F32),
        ],
        scratch_shapes=[
            pltpu.VMEM((total, width), BF16),
            pltpu.VMEM((nf * depth, packed), BF16),
            pltpu.VMEM((segments, lead + LEN, channels), F32),
            pltpu.SemaphoreType.DMA((nt + 2 + len(keys),)),
        ],
        cost_estimate=pl.CostEstimate(
            flops=2 * total * width * packed,
            transcendentals=total * channels,
            bytes_accessed=2 * width * packed,
        ),
        compiler_params=pltpu.CompilerParams(vmem_limit_bytes=24 * MEBI),
        name="glu_conv",
    )(spot, taps, *[blocks[d] for d in range(nt)], val, gate, *pieces.values())


def out_product(spot, sizes, conv, sums, gain, all_channels, own, pieces):
    ng, nf, nt = sizes
    total, channels = conv.shape
    rows = total // nt
    depth, cols = own.shape
    share = depth // ng
    keys = list(pieces)

    def run(spot_ref, conv_ref, gain_ref, *refs):
        sum_refs, refs = refs[: len(sums)], refs[len(sums) :]
        own_ref, refs = refs[0], refs[1:]
        piece_refs, refs = refs[: len(keys)], refs[len(keys) :]
        out_refs, refs = refs[:nt], refs[nt:]
        weight, mixed, sems = refs
        group, slab, member = spot_ref[0], spot_ref[1], spot_ref[2]
        pairs = [(own_ref, weight.at[slab])]
        for (d, e), ref in zip(keys, piece_refs):
            pairs.append((ref, weight.at[slab ^ d, aligned(group ^ e, share)]))
        copies = start_copies(pairs, sems)
        sums_all = sum(ref[...] for ref in sum_refs) * (1.0 / all_channels)
        row = lax.broadcasted_iota(jnp.int32, (total, total), 0)
        column = lax.broadcasted_iota(jnp.int32, (total, total), 1)

        def upright(line):
            return jnp.sum(jnp.where(row == column, line, 0.0), axis=1, keepdims=True)

        chan_mean = upright(sums_all[0:1, :])
        chan_var = upright(sums_all[8:9, :]) - chan_mean * chan_mean
        scaled = (conv_ref[...] - chan_mean) * lax.rsqrt(chan_var + chan_epsilon) * gain_ref[...]
        activated = (scaled * jax.nn.sigmoid(scaled)).astype(BF16)
        for copy in copies:
            copy.wait()
        outward = []
        for s in range(nf):
            columns = pl.ds(s * cols, cols)
            mixed[:, columns] = product(activated, weight[s]).astype(BF16)
            targets = [
                (mixed.at[aligned(member ^ d, rows), columns], out_refs[d].at[:, columns])
                for d in range(nt)
            ]
            outward += start_copies(targets, sems, 1 + len(keys) + len(outward))
        for copy in outward:
            copy.wait()

    return pl.pallas_call(
        run,
        in_specs=[SMEM, VMEM, VMEM] + [VMEM] * len(sums) + [HBM] + [ANY] * len(keys),
        out_specs=[ANY] * nt,
        out_shape=[jax.ShapeDtypeStruct((rows, nf * cols), BF16)] * nt,
        scratch_shapes=[
            pltpu.VMEM((nf, depth, cols), BF16),
            pltpu.VMEM((total, nf * cols), BF16),
            pltpu.SemaphoreType.DMA((1 + len(keys) + nf * nt,)),
        ],
        cost_estimate=pl.CostEstimate(
            flops=2 * total * channels * nf * cols,
            transcendentals=total * channels,
            bytes_accessed=2 * channels * nf * cols,
        ),
        compiler_params=pltpu.CompilerParams(vmem_limit_bytes=24 * MEBI),
        name="out_product",
    )(spot, conv, gain, *sums, own, *pieces.values())


def ffn_shares(spot, sizes, gate, val, down):
    ng, nf, _ = sizes
    depth, local_ff = gate.shape
    cols = down.shape[1]
    units = local_ff // nf
    whole = units // LANES * LANES
    rest = units - whole
    share = depth // ng
    packed = 2 * units
    count = nf - 1
    tall = (whole // ng, rest // ng)

    def run(spot_ref, *refs):
        sources, refs = refs[:3], refs[3:]
        out_refs, refs = refs[:count], refs[count:]
        up_own_ref, down_own_ref, gate_ref, val_ref, down_ref, halves, sems = refs
        group, slab = spot_ref[0], spot_ref[1]
        rows = aligned(group, share)
        for copy in start_copies(zip(sources, (gate_ref, val_ref, down_ref)), sems):
            copy.wait()
        mine = pl.ds(pl.multiple_of(slab * whole, LANES), whole)
        pairs = [
            (gate_ref.at[:, mine], up_own_ref.at[:, pl.ds(0, whole)]),
            (val_ref.at[:, mine], up_own_ref.at[:, pl.ds(whole, whole)]),
            (down_ref.at[mine], down_own_ref.at[pl.ds(0, whole)]),
        ]
        if rest:
            last = pl.ds(pl.multiple_of(nf * whole + slab * rest, 16), rest)
            pairs.append((down_ref.at[last], down_own_ref.at[pl.ds(whole, rest)]))
        for d in range(1, nf):
            there = slab ^ d
            columns = pl.ds(pl.multiple_of(there * whole, LANES), whole)
            out = out_refs[d - 1]
            for i, ref in enumerate((gate_ref, val_ref)):
                target = out.at[pl.ds(0, share), pl.ds(i * whole, whole)]
                pairs.append((ref.at[rows, columns], target))
            first = pl.multiple_of(there * whole + group * tall[0], 16)
            target = out.at[pl.ds(share, tall[0]), pl.ds(0, cols)]
            pairs.append((down_ref.at[pl.ds(first, tall[0])], target))
            first = pl.multiple_of(nf * whole + there * rest + group * tall[1], 16)
            for q in range(cols // LANES):
                source = down_ref.at[pl.ds(first, tall[1]), pl.ds(q * LANES, LANES)]
                target = out.at[pl.ds(share + q * tall[1], tall[1]), pl.ds(cols, LANES)]
                pairs.append((source, target))
        copies = start_copies(pairs, sems, 3)
        if rest:
            lane = lax.broadcasted_iota(jnp.int32, (depth, LANES), 1)
            for s in range(nf):
                begin = nf * whole + s * rest // LANES * LANES
                pair = [ref[:, begin : begin + LANES].astype(F32) for ref in (gate_ref, val_ref)]
                moved = 1 if s * rest % LANES == 0 else 0
                pair[moved] = pltpu.roll(pair[moved], rest, 1)
                halves[s] = jnp.where(lane < rest, pair[0], pair[1]).astype(BF16)
            pairs = [
                (
                    halves.at[slab ^ d, rows],
                    out_refs[d - 1].at[pl.ds(0, share), pl.ds(2 * whole, LANES)],
                )
                for d in range(1, nf)
            ]
            pairs.append((halves.at[slab], up_own_ref.at[:, pl.ds(2 * whole, LANES)]))
            copies += start_copies(pairs, sems, 3 + len(copies))
        for copy in copies:
            copy.wait()

    outs = pl.pallas_call(
        run,
        in_specs=[SMEM, HBM, HBM, HBM],
        out_specs=[ANY] * (count + 2),
        out_shape=[jax.ShapeDtypeStruct((share + tall[0], packed), BF16)] * count
        + [jax.ShapeDtypeStruct((depth, packed), BF16)]
        + [jax.ShapeDtypeStruct((units, cols), BF16)],
        scratch_shapes=[
            pltpu.VMEM(gate.shape, BF16),
            pltpu.VMEM(val.shape, BF16),
            pltpu.VMEM(down.shape, BF16),
            pltpu.VMEM((nf, depth, LANES), BF16),
            pltpu.SemaphoreType.DMA((8 + (4 + cols // LANES) * count,)),
        ],
        cost_estimate=pl.CostEstimate(
            flops=depth * packed, transcendentals=0, bytes_accessed=8 * depth * packed
        ),
        compiler_params=pltpu.CompilerParams(vmem_limit_bytes=60 * MEBI),
        name="ffn_shares",
    )(spot, gate, val, down)
    return {d: outs[d - 1] for d in range(1, nf)}, outs[-2], outs[-1]


def ffn_weights(spot, sizes, up_own, down_own, pieces):
    ng, nf, _ = sizes
    depth, packed = up_own.shape
    units, cols = down_own.shape
    whole = units // LANES * LANES
    rest = units - whole
    padded = -(-units // LANES) * LANES
    share = depth // ng
    tall = (whole // ng, rest // ng)
    keys = list(pieces)

    def run(spot_ref, up_own_ref, down_own_ref, *refs):
        piece_refs, refs = refs[: len(keys)], refs[len(keys) :]
        up, down, sems = refs
        group, slab = spot_ref[0], spot_ref[1]
        pairs = [
            (up_own_ref, up.at[aligned(slab, depth)]),
            (down_own_ref, down.at[slab, pl.ds(0, units)]),
        ]
        for (d, e), ref in zip(keys, piece_refs):
            place = (slab ^ d) * ng + (group ^ e)
            pairs.append((ref.at[pl.ds(0, share)], up.at[aligned(place, share)]))
            source = ref.at[pl.ds(share, tall[0]), pl.ds(0, cols)]
            pairs.append((source, down.at[slab ^ d, aligned(group ^ e, tall[0])]))
            first = pl.multiple_of(whole + (group ^ e) * tall[1], 16)
            for q in range(cols // LANES):
                source = ref.at[pl.ds(share + q * tall[1], tall[1]), pl.ds(cols, LANES)]
                target = down.at[slab ^ d, pl.ds(first, tall[1]), pl.ds(q * LANES, LANES)]
                pairs.append((source, target))
        copies = start_copies(pairs, sems)
        if padded > units:
            down[:, units:, :] = jnp.zeros((nf, padded - units, cols), BF16)
        for copy in copies:
            copy.wait()

    return pl.pallas_call(
        run,
        in_specs=[SMEM] + [ANY] * (2 + len(keys)),
        out_specs=[VMEM, VMEM],
        out_shape=[
            jax.ShapeDtypeStruct((nf * depth, packed), BF16),
            jax.ShapeDtypeStruct((nf, padded, cols), BF16),
        ],
        scratch_shapes=[pltpu.SemaphoreType.DMA((2 + (2 + cols // LANES) * len(keys),))],
        cost_estimate=pl.CostEstimate(
            flops=nf * depth * packed, transcendentals=0, bytes_accessed=4 * nf * depth * packed
        ),
        compiler_params=pltpu.CompilerParams(vmem_limit_bytes=12 * MEBI),
        name="ffn_weights",
    )(spot, up_own, down_own, *pieces.values())


def ffn_chunk(spot, sizes, blocks, up, taps, down):
    nt = sizes[2]
    rows, width = blocks[0].shape
    total = nt * rows
    packed = up.shape[1]
    parts, padded, cols = down.shape
    units = packed // 2
    whole = units // LANES * LANES
    rest = units - whole
    wide = 2 * LANES

    def run(spot_ref, taps_ref, up, down, *refs):
        block_refs, refs = refs[:nt], refs[nt:]
        out_refs, refs = refs[:nt], refs[nt:]
        gathered, hidden, mixed, sems = refs
        member = spot_ref[2]
        pairs = [(block_refs[d], gathered.at[aligned(member ^ d, rows)]) for d in range(nt)]
        for copy in start_copies(pairs, sems):
            copy.wait()

        def conv(column, size):
            raw = product(gathered[...], up[:, column : column + size])
            raw = raw.astype(BF16).astype(F32)
            place = lax.broadcasted_iota(jnp.int32, raw.shape, 0) % LEN
            span = taps_ref.shape[0]
            result = raw * taps_ref[span - 1 : span, column : column + size]
            for back in range(1, span):
                moved = jnp.where(place >= back, pltpu.roll(raw, back, 0), 0.0)
                tap = taps_ref[span - 1 - back : span - back, column : column + size]
                result = result + moved * tap
            return result

        def gelu(v):
            return 0.5 * v * (1.0 + jnp.tanh((2.0 / jnp.pi) ** 0.5 * (v + 0.044715 * v * v * v)))

        for column in range(0, whole, wide):
            size = min(wide, whole - column)
            gate, val = conv(column, size), conv(whole + column, size)
            hidden[:, column : column + size] = (gelu(gate) * val).astype(BF16)
        if rest:
            both = conv(2 * whole, LANES)
            lane = lax.broadcasted_iota(jnp.int32, both.shape, 1)
            gated = gelu(both) * pltpu.roll(both, LANES - rest, 1)
            hidden[:, whole:] = jnp.where(lane < rest, gated, 0.0).astype(BF16)
        outward = []
        for s in range(parts):
            columns = pl.ds(s * cols, cols)
            mixed[:, columns] = product(hidden[...], down[s]).astype(BF16)
            targets = [
                (mixed.at[aligned(member ^ d, rows), columns], out_refs[d].at[:, columns])
                for d in range(nt)
            ]
            outward += start_copies(targets, sems, nt + len(outward))
        for copy in outward:
            copy.wait()

    flops = 2 * total * width * packed + 2 * total * units * parts * cols
    return pl.pallas_call(
        run,
        in_specs=[SMEM, VMEM, VMEM, VMEM] + [ANY] * nt,
        out_specs=[ANY] * nt,
        out_shape=[jax.ShapeDtypeStruct((rows, parts * cols), BF16)] * nt,
        scratch_shapes=[
            pltpu.VMEM((total, width), BF16),
            pltpu.VMEM((total, padded), BF16),
            pltpu.VMEM((total, parts * cols), BF16),
            pltpu.SemaphoreType.DMA((nt + nt * parts,)),
        ],
        cost_estimate=pl.CostEstimate(
            flops=flops, transcendentals=total * units, bytes_accessed=2 * width * packed
        ),
        compiler_params=pltpu.CompilerParams(vmem_limit_bytes=20 * MEBI),
        name="ffn_chunk",
    )(spot, taps, up, down, *[blocks[d] for d in range(nt)])


def middle_pair(nf, d):
    return nf == 4 and d == nf - 1


def exchange_shards(sizes):
    ng, nf, nt = sizes

    def shards(
        tokens,
        mix_gain,
        val_weight,
        gate_weight,
        conv_taps,
        chan_gain,
        out_weight,
        mix_post_gain,
        ffn_gain,
        up_gate_weight,
        up_val_weight,
        ffn_taps,
        down_weight,
        ffn_post_gain,
    ):
        group, slab, member = (lax.axis_index(a) for a in ("grp", "fs", "tp"))
        spot = jnp.stack([group, slab, member]).astype(jnp.int32)

        def share_out(blocks):
            pieces = {(d, 0): blocks[d] for d in range(1, nf)}
            for d in range(1, nf):
                for e in range(1, ng):
                    pieces[d, e] = swap(blocks[d], "grp", ng, e)
            return pieces

        def fetch(shares, inner):
            sent = {}
            for d in shares:
                pairs = [(i, i ^ d) for i in range(nf)]
                early = [p for p in pairs if middle_pair(nf, d) and abs(p[0] - p[1]) == 1]
                late = [p for p in pairs if p not in early]
                sent[d] = lax.ppermute(shares[d], "fs", late)
                if early:
                    first = lax.ppermute(shares[d], "fs", early)
                    sent[d] = jnp.where(inner, first, sent[d])
            return share_out(sent)

        def fetch_all(mine):
            return share_out(gather_blocks(mine, "fs", nf))

        local_ch = val_weight.shape[1]
        glu_share = jnp.where(group == 0, val_weight, gate_weight)
        out_rows = out_weight.shape[0] // ng
        out_share = lax.dynamic_slice_in_dim(out_weight, group * out_rows, out_rows, 0)
        glu_pieces = fetch_all(glu_share)
        out_pieces = fetch_all(out_share)

        local_ff = up_gate_weight.shape[1]
        units = local_ff // nf
        whole = units // LANES * LANES
        rest = units - whole
        begin = member * local_ff
        taps_whole = lax.dynamic_slice_in_dim(ffn_taps, begin + slab * whole, whole, 2)
        own_taps = [taps_whole[0], taps_whole[1]]
        if rest:
            first = begin + nf * whole + slab * rest
            taps_rest = lax.dynamic_slice_in_dim(ffn_taps, first, rest, 2)
            own_taps += [taps_rest[0], taps_rest[1]]
        own_taps = jnp.concatenate(own_taps, axis=1).astype(F32)

        mix_taps = lax.dynamic_slice_in_dim(conv_taps, member * local_ch, local_ch, 1)
        own_gain = lax.dynamic_slice_in_dim(chan_gain[None], member * local_ch, local_ch, 1)
        mix_taps, own_gain = mix_taps.astype(F32), own_gain.astype(F32)
        post_gain, next_gain, last_gain = (
            gain[None] for gain in (mix_post_gain, ffn_gain, ffn_post_gain)
        )
        inner = (slab > 0) & (slab < nf - 1)
        small = (own_taps, mix_taps, own_gain, post_gain, next_gain, last_gain, inner)
        spot, small = lax.optimization_barrier((spot, small))
        own_taps, mix_taps, own_gain, post_gain, next_gain, last_gain, inner = small
        ffn_parts, up_own, down_own = ffn_shares(
            spot, sizes, up_gate_weight, up_val_weight, down_weight
        )
        ffn_pieces = fetch(ffn_parts, inner)
        up_full, down_full = ffn_weights(spot, sizes, up_own, down_own, ffn_pieces)

        def scaled(values, gain):
            mean = jnp.mean(values * values, axis=-1, keepdims=True)
            return values * lax.rsqrt(mean + norm_epsilon) * gain

        (normed,) = row_kernel(lambda t, g: (scaled(t, g),), [tokens, mix_gain[None]], 1)
        row_blocks = gather_blocks(normed, "tp", nt)
        conv, sums = glu_conv(
            spot, sizes, row_blocks, val_weight, gate_weight, glu_pieces, mix_taps
        )
        all_sums = [sums] + [swap(sums, "tp", nt, d) for d in range(1, nt)]
        mixed = out_product(
            spot,
            sizes,
            conv,
            all_sums,
            own_gain,
            chan_gain.shape[0],
            out_weight,
            out_pieces,
        )
        terms = scatter_blocks(dict(enumerate(mixed)), "tp", nt)

        def residual_rows(t, post, gain, *parts):
            result = (t + scaled(sum(parts), post)).astype(BF16).astype(F32)
            return result, scaled(result, gain)

        residual, acted = row_kernel(residual_rows, [tokens, post_gain, next_gain, *terms], 2)

        last = []
        acts = gather_blocks(acted, "fs", nf)
        for d in range(nf):
            blocks = gather_blocks(acts[d], "tp", nt)
            parts = ffn_chunk(spot, sizes, blocks, up_full, own_taps, down_full)
            terms = scatter_blocks(dict(enumerate(parts)), "tp", nt)
            if d:
                terms = [swap(add_terms(terms), "fs", nf, d)]
            last += terms
        (result,) = row_kernel(
            lambda r, gain, *parts: (r + scaled(sum(parts), gain),), [residual, last_gain, *last], 1
        )
        return result

    return shards


def gather_shards(
    tokens,
    mix_gain,
    val_weight,
    gate_weight,
    conv_taps,
    chan_gain,
    out_weight,
    mix_post_gain,
    ffn_gain,
    up_gate_weight,
    up_val_weight,
    ffn_taps,
    down_weight,
    ffn_post_gain,
):
    member = lax.axis_index("tp")
    normed_own = rms_scale(tokens.astype(jnp.float32), mix_gain).astype(jnp.bfloat16)
    normed = lax.all_gather(normed_own, "tp", axis=0, tiled=True)
    local_ch = val_weight.shape[1]
    values = product(normed, lax.all_gather(val_weight, "fs", axis=0, tiled=True))
    gate_sums = product(normed, lax.all_gather(gate_weight, "fs", axis=0, tiled=True))
    glu_out = (values * jax.nn.sigmoid(gate_sums)).astype(jnp.bfloat16)
    own_taps = lax.dynamic_slice_in_dim(conv_taps, member * local_ch, local_ch, 1)
    conv_out = depthwise(glu_out, own_taps)
    totals, squares = lax.psum(
        (jnp.sum(conv_out, axis=1), jnp.sum(conv_out * conv_out, axis=1)), "tp"
    )
    all_channels = chan_gain.shape[0]
    chan_mean = totals[:, None] / all_channels
    chan_var = squares[:, None] / all_channels - chan_mean * chan_mean
    own_gain = lax.dynamic_slice_in_dim(chan_gain, member * local_ch, local_ch, 0)
    scaled = (conv_out - chan_mean) * lax.rsqrt(chan_var + chan_epsilon)
    activated = jax.nn.silu(scaled * own_gain.astype(jnp.float32)).astype(jnp.bfloat16)
    out_full = lax.all_gather(out_weight, "fs", axis=1, tiled=True)
    mixed_sum = lax.psum_scatter(
        product(activated, out_full).astype(jnp.bfloat16), "tp", scatter_dimension=0, tiled=True
    ).astype(jnp.float32)
    residual = tokens.astype(jnp.float32) + rms_scale(mixed_sum, mix_post_gain)
    residual = residual.astype(jnp.bfloat16)
    normed_share = rms_scale(residual.astype(jnp.float32), ffn_gain).astype(jnp.bfloat16)
    normed_ffn = lax.all_gather(normed_share, "tp", axis=0, tiled=True)
    local_ff = up_gate_weight.shape[1]
    own_ffn_taps = lax.dynamic_slice_in_dim(ffn_taps, member * local_ff, local_ff, 2)
    gate_full = lax.all_gather(up_gate_weight, "fs", axis=0, tiled=True)
    val_full = lax.all_gather(up_val_weight, "fs", axis=0, tiled=True)
    up_gate = product(normed_ffn, gate_full).astype(jnp.bfloat16)
    up_val = product(normed_ffn, val_full).astype(jnp.bfloat16)
    gate_conv = depthwise(up_gate, own_ffn_taps[0])
    val_conv = depthwise(up_val, own_ffn_taps[1])
    hidden = (jax.nn.gelu(gate_conv, approximate=True) * val_conv).astype(jnp.bfloat16)
    down_full = lax.all_gather(down_weight, "fs", axis=1, tiled=True)
    ffn_sum = lax.psum_scatter(
        product(hidden, down_full).astype(jnp.bfloat16), "tp", scatter_dimension=0, tiled=True
    ).astype(jnp.float32)
    return (residual.astype(jnp.float32) + rms_scale(ffn_sum, ffn_post_gain)).astype(jnp.bfloat16)


def solution(mesh):
    sizes = tuple(mesh.shape[a] for a in ("grp", "fs", "tp"))
    specs = (
        P(("grp", "fs", "tp"), None),
        P(),
        P("fs", "tp"),
        P("fs", "tp"),
        P(),
        P(),
        P("tp", "fs"),
        P(),
        P(),
        P("fs", "tp"),
        P("fs", "tp"),
        P(),
        P("tp", "fs"),
        P(),
    )
    powers = all(size & (size - 1) == 0 for size in sizes)
    exchange = powers and sizes[0] == 2 and sizes[1] * sizes[2] <= 16

    def run(*args):
        units = args[9].shape[1] // (sizes[1] * sizes[2])
        cols = args[12].shape[1] // sizes[1]
        whole = units // LANES * LANES
        cuts = units - whole == LANES // 2 and cols + LANES == 2 * units
        cuts = cuts and cols // LANES * (units - whole) == whole and whole % (32 * sizes[0]) == 0
        shards = exchange_shards(sizes) if exchange and cuts else gather_shards
        return jax.shard_map(
            shards,
            mesh=mesh,
            in_specs=specs,
            out_specs=P(("grp", "fs", "tp"), None),
            check_vma=False,
        )(*args)

    return run
```

```python
import jax
import jax.numpy as jnp
from jax import lax
from jax.experimental import pallas as pl
from jax.experimental.pallas import tpu as pltpu
from jax.sharding import PartitionSpec as P

LEN = 64
LANES = 128
BF16 = jnp.bfloat16
F32 = jnp.float32
MEBI = 2**20

norm_epsilon = 1e-06
chan_epsilon = 1e-05


def rms_scale(values, gain):
    inverse = lax.rsqrt(jnp.mean(values * values, axis=-1, keepdims=True) + norm_epsilon)
    return values * inverse * gain.astype(jnp.float32)


def depthwise(signal, tap_table):
    taps_count = tap_table.shape[0]
    channels = signal.shape[1]
    shaped = signal.astype(jnp.float32).reshape(signal.shape[0] // LEN, LEN, channels)
    padded = jnp.pad(shaped, ((0, 0), (taps_count - 1, 0), (0, 0)))
    tap_values = tap_table.astype(jnp.float32)
    result = jnp.zeros(shaped.shape, jnp.float32)
    for offset in range(taps_count):
        result = result + padded[:, offset : offset + LEN, :] * tap_values[offset]
    return result.reshape(signal.shape[0], channels)


def product(left, weight):
    return jnp.dot(left, weight, preferred_element_type=jnp.float32)


def swap(array, axis, size, bits):
    return lax.ppermute(array, axis, [(i, i ^ bits) for i in range(size)])


def halvings(size):
    return [1 << b for b in reversed(range(size.bit_length() - 1))]


def gather_blocks(block, axis, size):
    blocks = {0: block}
    for bits in halvings(size):
        for d in list(blocks):
            blocks[d | bits] = swap(blocks[d], axis, size, bits)
    return blocks


def scatter_blocks(blocks, axis, size):
    terms = {d: [b] for d, b in blocks.items()}
    for bits in reversed(halvings(size)):
        kept = {}
        for d in terms:
            if not d & bits:
                sent = add_terms(terms[d | bits])
                other = swap(sent, axis, size, bits)
                kept[d] = [*terms[d], other]
        terms = kept
    return terms[0]


def add_terms(terms):
    if len(terms) == 1:
        return terms[0]
    return sum(t.astype(F32) for t in terms).astype(BF16)


VMEM = pl.BlockSpec(memory_space=pltpu.VMEM)
SMEM = pl.BlockSpec(memory_space=pltpu.SMEM)
ANY = pl.BlockSpec(memory_space=pl.ANY)
HBM = pl.BlockSpec(memory_space=pltpu.HBM)


def aligned(index, size):
    return pl.ds(pl.multiple_of(index * size, 16), size)


def start_copies(pairs, sems, first=0):
    copies = []
    for i, (source, target) in enumerate(pairs):
        copies.append(pltpu.make_async_copy(source, target, sems.at[first + i]))
        copies[-1].start()
    return copies


def row_kernel(body, arrays, outs):
    count = len(arrays)

    def run(*refs):
        results = body(*[ref[...].astype(F32) for ref in refs[:count]])
        for ref, result in zip(refs[count:], results):
            ref[...] = result.astype(ref.dtype)

    return pl.pallas_call(
        run,
        in_specs=[VMEM] * count,
        out_specs=[VMEM] * outs,
        out_shape=[jax.ShapeDtypeStruct(arrays[0].shape, BF16)] * outs,
        cost_estimate=pl.CostEstimate(
            flops=8 * arrays[0].size, transcendentals=0, bytes_accessed=4 * arrays[0].size
        ),
        compiler_params=pltpu.CompilerParams(vmem_limit_bytes=12 * MEBI),
    )(*arrays)


def glu_conv(spot, sizes, blocks, val, gate, pieces, taps):
    _, nf, nt = sizes
    rows, width = blocks[0].shape
    total = nt * rows
    depth, channels = val.shape
    packed = 2 * channels
    count = taps.shape[0]
    lead = -(-(count - 1) // 8) * 8
    segments = total // LEN
    keys = list(pieces)

    def run(spot_ref, taps_ref, *refs):
        block_refs, refs = refs[:nt], refs[nt:]
        own_refs, refs = refs[:2], refs[2:]
        piece_refs, refs = refs[: len(keys)], refs[len(keys) :]
        conv_ref, sums_ref, gathered, weight, padded, sems = refs
        group, slab, member = spot_ref[0], spot_ref[1], spot_ref[2]
        pairs = [(block_refs[d], gathered.at[aligned(member ^ d, rows)]) for d in range(nt)]
        for i, ref in enumerate(own_refs):
            columns = pl.ds(i * channels, channels)
            pairs.append((ref, weight.at[aligned(slab, depth), columns]))
        for (d, e), ref in zip(keys, piece_refs):
            columns = pl.ds(pl.multiple_of((group ^ e) * channels, LANES), channels)
            pairs.append((ref, weight.at[aligned(slab ^ d, depth), columns]))
        copies = start_copies(pairs, sems)
        padded[:, :lead, :] = jnp.zeros((segments, lead, channels), F32)
        for copy in copies:
            copy.wait()
        both = product(gathered[...], weight[...])
        glu = both[:, :channels] * jax.nn.sigmoid(both[:, channels:])
        glu = glu.astype(BF16).astype(F32)
        padded[:, lead:, :] = glu.reshape(segments, LEN, channels)

        def segment(s, carry):
            result = jnp.zeros((LEN, channels), F32)
            for k in range(count):
                begin = lead - (count - 1) + k
                result = result + padded[s, begin : begin + LEN, :] * taps_ref[k : k + 1, :]
            conv_ref[aligned(s, LEN), :] = result
            return carry

        lax.fori_loop(0, segments, segment, 0)
        conv = conv_ref[...]
        ones = jnp.ones((8, channels), F32)
        over = (((1,), (1,)), ((), ()))
        for i, term in enumerate((conv, conv * conv)):
            sums_ref[8 * i : 8 * i + 8, :] = lax.dot_general(
                ones, term, over, precision=lax.Precision.HIGHEST, preferred_element_type=F32
            )

    return pl.pallas_call(
        run,
        in_specs=[SMEM, VMEM] + [ANY] * nt + [HBM] * 2 + [ANY] * len(keys),
        out_specs=[VMEM, VMEM],
        out_shape=[
            jax.ShapeDtypeStruct((total, channels), F32),
            jax.ShapeDtypeStruct((16, total), F32),
        ],
        scratch_shapes=[
            pltpu.VMEM((total, width), BF16),
            pltpu.VMEM((nf * depth, packed), BF16),
            pltpu.VMEM((segments, lead + LEN, channels), F32),
            pltpu.SemaphoreType.DMA((nt + 2 + len(keys),)),
        ],
        cost_estimate=pl.CostEstimate(
            flops=2 * total * width * packed,
            transcendentals=total * channels,
            bytes_accessed=2 * width * packed,
        ),
        compiler_params=pltpu.CompilerParams(vmem_limit_bytes=24 * MEBI),
        name="glu_conv",
    )(spot, taps, *[blocks[d] for d in range(nt)], val, gate, *pieces.values())


def out_product(spot, sizes, conv, sums, gain, all_channels, own, pieces):
    ng, nf, nt = sizes
    total, channels = conv.shape
    rows = total // nt
    depth, cols = own.shape
    share = depth // ng
    keys = list(pieces)

    def run(spot_ref, conv_ref, gain_ref, *refs):
        sum_refs, refs = refs[: len(sums)], refs[len(sums) :]
        own_ref, refs = refs[0], refs[1:]
        piece_refs, refs = refs[: len(keys)], refs[len(keys) :]
        out_refs, refs = refs[:nt], refs[nt:]
        weight, mixed, sems = refs
        group, slab, member = spot_ref[0], spot_ref[1], spot_ref[2]
        pairs = [(own_ref, weight.at[slab])]
        for (d, e), ref in zip(keys, piece_refs):
            pairs.append((ref, weight.at[slab ^ d, aligned(group ^ e, share)]))
        copies = start_copies(pairs, sems)
        sums_all = sum(ref[...] for ref in sum_refs) * (1.0 / all_channels)
        row = lax.broadcasted_iota(jnp.int32, (total, total), 0)
        column = lax.broadcasted_iota(jnp.int32, (total, total), 1)

        def upright(line):
            return jnp.sum(jnp.where(row == column, line, 0.0), axis=1, keepdims=True)

        chan_mean = upright(sums_all[0:1, :])
        chan_var = upright(sums_all[8:9, :]) - chan_mean * chan_mean
        scaled = (conv_ref[...] - chan_mean) * lax.rsqrt(chan_var + chan_epsilon) * gain_ref[...]
        activated = (scaled * jax.nn.sigmoid(scaled)).astype(BF16)
        for copy in copies:
            copy.wait()
        for s in range(nf):
            mixed[:, s * cols : (s + 1) * cols] = product(activated, weight[s]).astype(BF16)
        targets = [(mixed.at[aligned(member ^ d, rows)], out_refs[d]) for d in range(nt)]
        for copy in start_copies(targets, sems):
            copy.wait()

    return pl.pallas_call(
        run,
        in_specs=[SMEM, VMEM, VMEM] + [VMEM] * len(sums) + [HBM] + [ANY] * len(keys),
        out_specs=[ANY] * nt,
        out_shape=[jax.ShapeDtypeStruct((rows, nf * cols), BF16)] * nt,
        scratch_shapes=[
            pltpu.VMEM((nf, depth, cols), BF16),
            pltpu.VMEM((total, nf * cols), BF16),
            pltpu.SemaphoreType.DMA((1 + len(keys) + nf * nt,)),
        ],
        cost_estimate=pl.CostEstimate(
            flops=2 * total * channels * nf * cols,
            transcendentals=total * channels,
            bytes_accessed=2 * channels * nf * cols,
        ),
        compiler_params=pltpu.CompilerParams(vmem_limit_bytes=24 * MEBI),
        name="out_product",
    )(spot, conv, gain, *sums, own, *pieces.values())


def ffn_shares(spot, sizes, gate, val, down):
    ng, nf, _ = sizes
    depth, local_ff = gate.shape
    cols = down.shape[1]
    units = local_ff // nf
    whole = units // LANES * LANES
    rest = units - whole
    share = depth // ng
    packed = 2 * units
    count = nf - 1
    tall = (whole // ng, rest // ng)

    def run(spot_ref, *refs):
        sources, refs = refs[:3], refs[3:]
        out_refs, refs = refs[:count], refs[count:]
        up_own_ref, down_own_ref, gate_ref, val_ref, down_ref, halves, sems = refs
        group, slab = spot_ref[0], spot_ref[1]
        rows = aligned(group, share)
        for copy in start_copies(zip(sources, (gate_ref, val_ref, down_ref)), sems):
            copy.wait()
        mine = pl.ds(pl.multiple_of(slab * whole, LANES), whole)
        pairs = [
            (gate_ref.at[:, mine], up_own_ref.at[:, pl.ds(0, whole)]),
            (val_ref.at[:, mine], up_own_ref.at[:, pl.ds(whole, whole)]),
            (down_ref.at[mine], down_own_ref.at[pl.ds(0, whole)]),
        ]
        if rest:
            last = pl.ds(pl.multiple_of(nf * whole + slab * rest, 16), rest)
            pairs.append((down_ref.at[last], down_own_ref.at[pl.ds(whole, rest)]))
        for d in range(1, nf):
            there = slab ^ d
            columns = pl.ds(pl.multiple_of(there * whole, LANES), whole)
            out = out_refs[d - 1]
            for i, ref in enumerate((gate_ref, val_ref)):
                target = out.at[pl.ds(0, share), pl.ds(i * whole, whole)]
                pairs.append((ref.at[rows, columns], target))
            first = pl.multiple_of(there * whole + group * tall[0], 16)
            target = out.at[pl.ds(share, tall[0]), pl.ds(0, cols)]
            pairs.append((down_ref.at[pl.ds(first, tall[0])], target))
            first = pl.multiple_of(nf * whole + there * rest + group * tall[1], 16)
            for q in range(cols // LANES):
                source = down_ref.at[pl.ds(first, tall[1]), pl.ds(q * LANES, LANES)]
                target = out.at[pl.ds(share + q * tall[1], tall[1]), pl.ds(cols, LANES)]
                pairs.append((source, target))
        copies = start_copies(pairs, sems, 3)
        if rest:
            lane = lax.broadcasted_iota(jnp.int32, (depth, LANES), 1)
            for s in range(nf):
                begin = nf * whole + s * rest // LANES * LANES
                pair = [ref[:, begin : begin + LANES].astype(F32) for ref in (gate_ref, val_ref)]
                moved = 1 if s * rest % LANES == 0 else 0
                pair[moved] = pltpu.roll(pair[moved], rest, 1)
                halves[s] = jnp.where(lane < rest, pair[0], pair[1]).astype(BF16)
            pairs = [
                (
                    halves.at[slab ^ d, rows],
                    out_refs[d - 1].at[pl.ds(0, share), pl.ds(2 * whole, LANES)],
                )
                for d in range(1, nf)
            ]
            pairs.append((halves.at[slab], up_own_ref.at[:, pl.ds(2 * whole, LANES)]))
            copies += start_copies(pairs, sems, 3 + len(copies))
        for copy in copies:
            copy.wait()

    outs = pl.pallas_call(
        run,
        in_specs=[SMEM, HBM, HBM, HBM],
        out_specs=[ANY] * (count + 2),
        out_shape=[jax.ShapeDtypeStruct((share + tall[0], packed), BF16)] * count
        + [jax.ShapeDtypeStruct((depth, packed), BF16)]
        + [jax.ShapeDtypeStruct((units, cols), BF16)],
        scratch_shapes=[
            pltpu.VMEM(gate.shape, BF16),
            pltpu.VMEM(val.shape, BF16),
            pltpu.VMEM(down.shape, BF16),
            pltpu.VMEM((nf, depth, LANES), BF16),
            pltpu.SemaphoreType.DMA((8 + (4 + cols // LANES) * count,)),
        ],
        cost_estimate=pl.CostEstimate(
            flops=depth * packed, transcendentals=0, bytes_accessed=8 * depth * packed
        ),
        compiler_params=pltpu.CompilerParams(vmem_limit_bytes=60 * MEBI),
        name="ffn_shares",
    )(spot, gate, val, down)
    return {d: outs[d - 1] for d in range(1, nf)}, outs[-2], outs[-1]


def ffn_weights(spot, sizes, up_own, down_own, pieces):
    ng, nf, _ = sizes
    depth, packed = up_own.shape
    units, cols = down_own.shape
    whole = units // LANES * LANES
    rest = units - whole
    padded = -(-units // LANES) * LANES
    share = depth // ng
    tall = (whole // ng, rest // ng)
    keys = list(pieces)

    def run(spot_ref, up_own_ref, down_own_ref, *refs):
        piece_refs, refs = refs[: len(keys)], refs[len(keys) :]
        up, down, sems = refs
        group, slab = spot_ref[0], spot_ref[1]
        pairs = [
            (up_own_ref, up.at[aligned(slab, depth)]),
            (down_own_ref, down.at[slab, pl.ds(0, units)]),
        ]
        for (d, e), ref in zip(keys, piece_refs):
            place = (slab ^ d) * ng + (group ^ e)
            pairs.append((ref.at[pl.ds(0, share)], up.at[aligned(place, share)]))
            source = ref.at[pl.ds(share, tall[0]), pl.ds(0, cols)]
            pairs.append((source, down.at[slab ^ d, aligned(group ^ e, tall[0])]))
            first = pl.multiple_of(whole + (group ^ e) * tall[1], 16)
            for q in range(cols // LANES):
                source = ref.at[pl.ds(share + q * tall[1], tall[1]), pl.ds(cols, LANES)]
                target = down.at[slab ^ d, pl.ds(first, tall[1]), pl.ds(q * LANES, LANES)]
                pairs.append((source, target))
        copies = start_copies(pairs, sems)
        if padded > units:
            down[:, units:, :] = jnp.zeros((nf, padded - units, cols), BF16)
        for copy in copies:
            copy.wait()

    return pl.pallas_call(
        run,
        in_specs=[SMEM] + [ANY] * (2 + len(keys)),
        out_specs=[VMEM, VMEM],
        out_shape=[
            jax.ShapeDtypeStruct((nf * depth, packed), BF16),
            jax.ShapeDtypeStruct((nf, padded, cols), BF16),
        ],
        scratch_shapes=[pltpu.SemaphoreType.DMA((2 + (2 + cols // LANES) * len(keys),))],
        cost_estimate=pl.CostEstimate(
            flops=nf * depth * packed, transcendentals=0, bytes_accessed=4 * nf * depth * packed
        ),
        compiler_params=pltpu.CompilerParams(vmem_limit_bytes=12 * MEBI),
        name="ffn_weights",
    )(spot, up_own, down_own, *pieces.values())


def ffn_chunk(spot, sizes, blocks, up, taps, down):
    nt = sizes[2]
    rows, width = blocks[0].shape
    total = nt * rows
    packed = up.shape[1]
    parts, padded, cols = down.shape
    units = packed // 2
    whole = units // LANES * LANES
    rest = units - whole
    wide = 2 * LANES

    def run(spot_ref, taps_ref, up, down, *refs):
        block_refs, refs = refs[:nt], refs[nt:]
        out_refs, refs = refs[:nt], refs[nt:]
        gathered, hidden, mixed = refs
        member = spot_ref[2]
        for d in range(nt):
            gathered[aligned(member ^ d, rows), :] = block_refs[d][...]

        def conv(column, size):
            raw = product(gathered[...], up[:, column : column + size])
            raw = raw.astype(BF16).astype(F32)
            place = lax.broadcasted_iota(jnp.int32, raw.shape, 0) % LEN
            span = taps_ref.shape[0]
            result = raw * taps_ref[span - 1 : span, column : column + size]
            for back in range(1, span):
                moved = jnp.where(place >= back, pltpu.roll(raw, back, 0), 0.0)
                tap = taps_ref[span - 1 - back : span - back, column : column + size]
                result = result + moved * tap
            return result

        def gelu(v):
            return 0.5 * v * (1.0 + jnp.tanh((2.0 / jnp.pi) ** 0.5 * (v + 0.044715 * v * v * v)))

        for column in range(0, whole, wide):
            size = min(wide, whole - column)
            gate, val = conv(column, size), conv(whole + column, size)
            hidden[:, column : column + size] = (gelu(gate) * val).astype(BF16)
        if rest:
            both = conv(2 * whole, LANES)
            lane = lax.broadcasted_iota(jnp.int32, both.shape, 1)
            gated = gelu(both) * pltpu.roll(both, LANES - rest, 1)
            hidden[:, whole:] = jnp.where(lane < rest, gated, 0.0).astype(BF16)
        for s in range(parts):
            mixed[:, s * cols : (s + 1) * cols] = product(hidden[...], down[s]).astype(BF16)
        for d in range(nt):
            out_refs[d][...] = mixed[aligned(member ^ d, rows), :]

    flops = 2 * total * width * packed + 2 * total * units * parts * cols
    return pl.pallas_call(
        run,
        in_specs=[SMEM, VMEM, VMEM, VMEM] + [VMEM] * nt,
        out_specs=[VMEM] * nt,
        out_shape=[jax.ShapeDtypeStruct((rows, parts * cols), BF16)] * nt,
        scratch_shapes=[
            pltpu.VMEM((total, width), BF16),
            pltpu.VMEM((total, padded), BF16),
            pltpu.VMEM((total, parts * cols), BF16),
        ],
        cost_estimate=pl.CostEstimate(
            flops=flops, transcendentals=total * units, bytes_accessed=2 * width * packed
        ),
        compiler_params=pltpu.CompilerParams(vmem_limit_bytes=20 * MEBI),
        name="ffn_chunk",
    )(spot, taps, up, down, *[blocks[d] for d in range(nt)])


def middle_pair(nf, d):
    return nf == 4 and d == nf - 1


def exchange_shards(sizes):
    ng, nf, nt = sizes

    def shards(
        tokens,
        mix_gain,
        val_weight,
        gate_weight,
        conv_taps,
        chan_gain,
        out_weight,
        mix_post_gain,
        ffn_gain,
        up_gate_weight,
        up_val_weight,
        ffn_taps,
        down_weight,
        ffn_post_gain,
    ):
        group, slab, member = (lax.axis_index(a) for a in ("grp", "fs", "tp"))
        spot = jnp.stack([group, slab, member]).astype(jnp.int32)

        def share_out(blocks):
            pieces = {(d, 0): blocks[d] for d in range(1, nf)}
            for d in range(1, nf):
                for e in range(1, ng):
                    pieces[d, e] = swap(blocks[d], "grp", ng, e)
            return pieces

        def fetch(shares, inner):
            sent = {}
            for d in shares:
                pairs = [(i, i ^ d) for i in range(nf)]
                early = [p for p in pairs if middle_pair(nf, d) and abs(p[0] - p[1]) == 1]
                late = [p for p in pairs if p not in early]
                sent[d] = lax.ppermute(shares[d], "fs", late)
                if early:
                    first = lax.ppermute(shares[d], "fs", early)
                    sent[d] = jnp.where(inner, first, sent[d])
            return share_out(sent)

        def fetch_all(mine):
            return share_out(gather_blocks(mine, "fs", nf))

        local_ch = val_weight.shape[1]
        glu_share = jnp.where(group == 0, val_weight, gate_weight)
        out_rows = out_weight.shape[0] // ng
        out_share = lax.dynamic_slice_in_dim(out_weight, group * out_rows, out_rows, 0)
        glu_pieces = fetch_all(glu_share)
        out_pieces = fetch_all(out_share)

        local_ff = up_gate_weight.shape[1]
        units = local_ff // nf
        whole = units // LANES * LANES
        rest = units - whole
        begin = member * local_ff
        taps_whole = lax.dynamic_slice_in_dim(ffn_taps, begin + slab * whole, whole, 2)
        own_taps = [taps_whole[0], taps_whole[1]]
        if rest:
            first = begin + nf * whole + slab * rest
            taps_rest = lax.dynamic_slice_in_dim(ffn_taps, first, rest, 2)
            own_taps += [taps_rest[0], taps_rest[1]]
        own_taps = jnp.concatenate(own_taps, axis=1).astype(F32)

        mix_taps = lax.dynamic_slice_in_dim(conv_taps, member * local_ch, local_ch, 1)
        own_gain = lax.dynamic_slice_in_dim(chan_gain[None], member * local_ch, local_ch, 1)
        mix_taps, own_gain = mix_taps.astype(F32), own_gain.astype(F32)
        post_gain, next_gain, last_gain = (
            gain[None] for gain in (mix_post_gain, ffn_gain, ffn_post_gain)
        )
        inner = (slab > 0) & (slab < nf - 1)
        small = (own_taps, mix_taps, own_gain, post_gain, next_gain, last_gain, inner)
        spot, small = lax.optimization_barrier((spot, small))
        own_taps, mix_taps, own_gain, post_gain, next_gain, last_gain, inner = small
        ffn_parts, up_own, down_own = ffn_shares(
            spot, sizes, up_gate_weight, up_val_weight, down_weight
        )
        ffn_pieces = fetch(ffn_parts, inner)
        up_full, down_full = ffn_weights(spot, sizes, up_own, down_own, ffn_pieces)

        def scaled(values, gain):
            mean = jnp.mean(values * values, axis=-1, keepdims=True)
            return values * lax.rsqrt(mean + norm_epsilon) * gain

        (normed,) = row_kernel(lambda t, g: (scaled(t, g),), [tokens, mix_gain[None]], 1)
        row_blocks = gather_blocks(normed, "tp", nt)
        conv, sums = glu_conv(
            spot, sizes, row_blocks, val_weight, gate_weight, glu_pieces, mix_taps
        )
        all_sums = [sums] + [swap(sums, "tp", nt, d) for d in range(1, nt)]
        mixed = out_product(
            spot,
            sizes,
            conv,
            all_sums,
            own_gain,
            chan_gain.shape[0],
            out_weight,
            out_pieces,
        )
        terms = scatter_blocks(dict(enumerate(mixed)), "tp", nt)

        def residual_rows(t, post, gain, *parts):
            result = (t + scaled(sum(parts), post)).astype(BF16).astype(F32)
            return result, scaled(result, gain)

        residual, acted = row_kernel(residual_rows, [tokens, post_gain, next_gain, *terms], 2)

        last = []
        acts = gather_blocks(acted, "fs", nf)
        for d in range(nf):
            blocks = gather_blocks(acts[d], "tp", nt)
            parts = ffn_chunk(spot, sizes, blocks, up_full, own_taps, down_full)
            terms = scatter_blocks(dict(enumerate(parts)), "tp", nt)
            if d:
                terms = [swap(add_terms(terms), "fs", nf, d)]
            last += terms
        (result,) = row_kernel(
            lambda r, gain, *parts: (r + scaled(sum(parts), gain),), [residual, last_gain, *last], 1
        )
        return result

    return shards


def gather_shards(
    tokens,
    mix_gain,
    val_weight,
    gate_weight,
    conv_taps,
    chan_gain,
    out_weight,
    mix_post_gain,
    ffn_gain,
    up_gate_weight,
    up_val_weight,
    ffn_taps,
    down_weight,
    ffn_post_gain,
):
    member = lax.axis_index("tp")
    normed_own = rms_scale(tokens.astype(jnp.float32), mix_gain).astype(jnp.bfloat16)
    normed = lax.all_gather(normed_own, "tp", axis=0, tiled=True)
    local_ch = val_weight.shape[1]
    values = product(normed, lax.all_gather(val_weight, "fs", axis=0, tiled=True))
    gate_sums = product(normed, lax.all_gather(gate_weight, "fs", axis=0, tiled=True))
    glu_out = (values * jax.nn.sigmoid(gate_sums)).astype(jnp.bfloat16)
    own_taps = lax.dynamic_slice_in_dim(conv_taps, member * local_ch, local_ch, 1)
    conv_out = depthwise(glu_out, own_taps)
    totals, squares = lax.psum(
        (jnp.sum(conv_out, axis=1), jnp.sum(conv_out * conv_out, axis=1)), "tp"
    )
    all_channels = chan_gain.shape[0]
    chan_mean = totals[:, None] / all_channels
    chan_var = squares[:, None] / all_channels - chan_mean * chan_mean
    own_gain = lax.dynamic_slice_in_dim(chan_gain, member * local_ch, local_ch, 0)
    scaled = (conv_out - chan_mean) * lax.rsqrt(chan_var + chan_epsilon)
    activated = jax.nn.silu(scaled * own_gain.astype(jnp.float32)).astype(jnp.bfloat16)
    out_full = lax.all_gather(out_weight, "fs", axis=1, tiled=True)
    mixed_sum = lax.psum_scatter(
        product(activated, out_full).astype(jnp.bfloat16), "tp", scatter_dimension=0, tiled=True
    ).astype(jnp.float32)
    residual = tokens.astype(jnp.float32) + rms_scale(mixed_sum, mix_post_gain)
    residual = residual.astype(jnp.bfloat16)
    normed_share = rms_scale(residual.astype(jnp.float32), ffn_gain).astype(jnp.bfloat16)
    normed_ffn = lax.all_gather(normed_share, "tp", axis=0, tiled=True)
    local_ff = up_gate_weight.shape[1]
    own_ffn_taps = lax.dynamic_slice_in_dim(ffn_taps, member * local_ff, local_ff, 2)
    gate_full = lax.all_gather(up_gate_weight, "fs", axis=0, tiled=True)
    val_full = lax.all_gather(up_val_weight, "fs", axis=0, tiled=True)
    up_gate = product(normed_ffn, gate_full).astype(jnp.bfloat16)
    up_val = product(normed_ffn, val_full).astype(jnp.bfloat16)
    gate_conv = depthwise(up_gate, own_ffn_taps[0])
    val_conv = depthwise(up_val, own_ffn_taps[1])
    hidden = (jax.nn.gelu(gate_conv, approximate=True) * val_conv).astype(jnp.bfloat16)
    down_full = lax.all_gather(down_weight, "fs", axis=1, tiled=True)
    ffn_sum = lax.psum_scatter(
        product(hidden, down_full).astype(jnp.bfloat16), "tp", scatter_dimension=0, tiled=True
    ).astype(jnp.float32)
    return (residual.astype(jnp.float32) + rms_scale(ffn_sum, ffn_post_gain)).astype(jnp.bfloat16)


def solution(mesh):
    sizes = tuple(mesh.shape[a] for a in ("grp", "fs", "tp"))
    specs = (
        P(("grp", "fs", "tp"), None),
        P(),
        P("fs", "tp"),
        P("fs", "tp"),
        P(),
        P(),
        P("tp", "fs"),
        P(),
        P(),
        P("fs", "tp"),
        P("fs", "tp"),
        P(),
        P("tp", "fs"),
        P(),
    )
    powers = all(size & (size - 1) == 0 for size in sizes)
    exchange = powers and sizes[0] == 2 and sizes[1] * sizes[2] <= 16

    def run(*args):
        units = args[9].shape[1] // (sizes[1] * sizes[2])
        cols = args[12].shape[1] // sizes[1]
        whole = units // LANES * LANES
        cuts = units - whole == LANES // 2 and cols + LANES == 2 * units
        cuts = cuts and cols // LANES * (units - whole) == whole and whole % (32 * sizes[0]) == 0
        shards = exchange_shards(sizes) if exchange and cuts else gather_shards
        return jax.shard_map(
            shards,
            mesh=mesh,
            in_specs=specs,
            out_specs=P(("grp", "fs", "tp"), None),
            check_vma=False,
        )(*args)

    return run
```
